256 devices in a mesh: sp: 64 (over z, x, core), tp: 4 (over y).
Axes of the slice: x: 4, y: 4, z: 8, core: 2. Of those that a mesh axis runs over, the one named last changes fastest.
Arguments:
- tokens: bfloat16 [16384, 2048], P(('sp', 'tp')), may hold values from -6 to 6
- norm_gain: float32 [2048], replicated, may hold values from 0.1 to 1.9
- w_glu_a: bfloat16 [2048, 2048], P(None, 'tp'), may hold values from -0.125 to 0.125
- w_glu_b: bfloat16 [2048, 2048], P(None, 'tp'), may hold values from -0.125 to 0.125
- conv_taps: float32 [31, 2048], P(None, 'tp'), may hold values from -6 to 6
- ln_gain: float32 [2048], P('tp'), may hold values from 0.1 to 1.9
- w_query: bfloat16 [2048, 2048], P(None, 'tp'), may hold values from -0.125 to 0.125
- w_key: bfloat16 [2048, 512], P(None, 'tp'), may hold values from -0.125 to 0.125
- w_value: bfloat16 [2048, 512], P(None, 'tp'), may hold values from -0.125 to 0.125
- query_gain: float32 [16, 128], P('tp'), may hold values from 1 to 40
- key_gain: float32 [4, 128], P('tp'), may hold values from 0.1 to 1.9
- lam_head: float32 [16], P('tp'), may hold values from 0.3 to 0.8
- sub_gain: float32 [128], replicated, may hold values from 0.1 to 1.9
- w_out_conv: bfloat16 [2048, 2048], P('tp'), may hold values from -0.09375 to 0.09375
- w_out_attn: bfloat16 [2048, 2048], P('tp'), may hold values from -0.09375 to 0.09375
Outputs:
- mixed: bfloat16 [16384, 2048], P(('sp', 'tp'))
- log_sums: float32 [2, 16, 16384], P(None, 'tp', 'sp')
The draws below stay inside these ranges and needn't reach their ends.
All inputs are finite; a program needn't handle non-finite values.
Results may differ from the reference program's by a relative error of at most 0.015.
The reference program's roundings to bfloat16 on the way count: a program that leaves them out, or rounds other values in their place, can miss the bound.
Values may be sent and summed in bfloat16 or wider, within the bound.
A program may use at most 128 MiB of HBM per device.

```python
import jax
import jax.numpy as jnp
from jax import lax

D = 2048
CONV_CH = 2048
KW = 31
HEADS = 16
KV_HEADS = 4
HEAD_DIM = 64
VALUE_DIM = 128
TOKENS = 16384
N_TP = 4


def draw_conv_taps(key, part):
    normal_part = jax.random.truncated_normal(key, -3.0, 3.0, (KW, CONV_CH), jnp.float32)
    channel_pos = jnp.arange(CONV_CH, dtype=jnp.float32) / CONV_CH
    growth = 3.0
    return normal_part * KW ** (-0.5) * jnp.exp(jnp.log(growth) * channel_pos)[None, :]


def draw_query_gain(key, part):
    gains = jax.random.uniform(key, (HEADS, 2 * HEAD_DIM), jnp.float32, 1.2, 1.9)
    return gains


def level_of(rng, extent, pieces, least, largest):
    def one(axis_at, blocks):
        draws = jax.random.uniform(jax.random.fold_in(jax.random.fold_in(rng, 6), axis_at), (blocks,), jnp.float32, least / len(pieces), largest / len(pieces))
        return jnp.repeat(jnp.exp(draws), extent[axis_at] // blocks).reshape((-1,) + (1,) * (len(extent) - axis_at - 1))

    loudness = one(*pieces[0])
    for cut in pieces[1:]:
        loudness = loudness * one(*cut)
    return loudness


def normal_values(key, shape, scale, reach, cuts=(), kind=jnp.bfloat16):
    factor_of = level_of(key, shape, cuts, -0.22, 0.18) if cuts else 1.0
    drawn = jax.random.normal(key, shape, jnp.float32) * scale * factor_of
    return jnp.minimum(jnp.maximum(drawn, -reach), reach).astype(kind)


def setup_inputs(seed: int = 0) -> dict:
    key_list = jax.random.split(jax.random.key(seed), 16)
    return {
        "tokens": normal_values(key_list[0], (TOKENS, D), 1.0, 6.0, ((0, 256),)),
        "norm_gain": jnp.clip(1.0 + 0.18 * jax.random.normal(key_list[1], (D,), jnp.float32), 0.1, 1.9),
        "w_glu_a": normal_values(key_list[2], (D, CONV_CH), D ** -0.5, 0.125, ((1, 4),)),
        "w_glu_b": normal_values(key_list[3], (D, CONV_CH), D ** -0.5, 0.125, ((1, 4),)),
        "conv_taps": draw_conv_taps(jax.random.fold_in(key_list[15], 71), 0),
        "ln_gain": jnp.clip(1.0 + 0.18 * jax.random.normal(key_list[5], (CONV_CH,), jnp.float32), 0.1, 1.9),
        "w_query": normal_values(key_list[6], (D, HEADS * 2 * HEAD_DIM), D ** -0.5, 0.125, ((1, 4),)),
        "w_key": normal_values(key_list[7], (D, KV_HEADS * 2 * HEAD_DIM), D ** -0.5, 0.125, ((1, 4),)),
        "w_value": normal_values(key_list[8], (D, KV_HEADS * VALUE_DIM), D ** -0.5, 0.125, ((1, 4),)),
        "query_gain": draw_query_gain(jax.random.fold_in(key_list[15], 71), 0),
        "key_gain": jnp.clip(1.0 + 0.18 * jax.random.normal(key_list[10], (KV_HEADS, 2 * HEAD_DIM), jnp.float32), 0.1, 1.9),
        "lam_head": jnp.clip(0.3 + 0.5 * jax.random.uniform(key_list[11], (HEADS,), jnp.float32) ** level_of(key_list[11], (HEADS,), ((0, 4),), -0.2, 0.2), 0.3, 0.8),
        "sub_gain": jnp.clip(1.0 + 0.18 * jax.random.normal(key_list[12], (VALUE_DIM,), jnp.float32), 0.1, 1.9),
        "w_out_conv": normal_values(key_list[13], (CONV_CH, D), (CONV_CH + HEADS * VALUE_DIM) ** -0.5, 0.09375, ((0, 4),)),
        "w_out_attn": normal_values(key_list[14], (HEADS * VALUE_DIM, D), (CONV_CH + HEADS * VALUE_DIM) ** -0.5, 0.09375, ((0, 4),)),
    }


def rms_scale(inputs_arr, gain_vec, epsilon):
    return inputs_arr * lax.rsqrt(lax.optimization_barrier(jnp.mean(inputs_arr * inputs_arr, axis=-1, keepdims=True)) + epsilon) * gain_vec

def reference(tokens, norm_gain, w_glu_a, w_glu_b, conv_taps, ln_gain, w_query, w_key, w_value, query_gain, key_gain, lam_head, sub_gain, w_out_conv, w_out_attn):
    seq_len = tokens.shape[0]
    normed = rms_scale(tokens.astype(jnp.float32), norm_gain, 1e-06).astype(jnp.bfloat16)
    glu_a = jnp.dot(normed, w_glu_a, preferred_element_type=jnp.float32)
    glu_b = jnp.dot(normed, w_glu_b, preferred_element_type=jnp.float32)
    gated_rows = (glu_a * jax.nn.sigmoid(glu_b)).astype(jnp.bfloat16)
    padded = jnp.concatenate([jnp.zeros((KW - 1, CONV_CH), jnp.bfloat16), gated_rows], axis=0)
    conv_sum = jnp.zeros((seq_len, CONV_CH), jnp.float32)
    for tap_idx in range(KW):
        conv_sum = conv_sum + conv_taps[tap_idx] * padded[tap_idx:tap_idx + seq_len].astype(jnp.float32)
    mean_val = lax.optimization_barrier(jnp.mean(conv_sum, axis=1, keepdims=True))
    mean_sq = lax.optimization_barrier(jnp.mean(conv_sum * conv_sum, axis=1, keepdims=True))
    normed_conv = (conv_sum - mean_val) * lax.rsqrt(mean_sq - mean_val * mean_val + 1e-05) * ln_gain
    conv_out = jax.nn.silu(normed_conv).astype(jnp.bfloat16)
    queries = jnp.dot(normed, w_query, preferred_element_type=jnp.float32).reshape(seq_len, HEADS, 2, HEAD_DIM)
    queries = rms_scale(queries, query_gain.reshape(HEADS, 2, HEAD_DIM), 1e-06).astype(jnp.bfloat16)
    key_heads = jnp.dot(normed, w_key, preferred_element_type=jnp.float32).reshape(seq_len, KV_HEADS, 2, HEAD_DIM)
    key_heads = rms_scale(key_heads, key_gain.reshape(KV_HEADS, 2, HEAD_DIM), 1e-06).astype(jnp.bfloat16)
    value_heads = jnp.dot(normed, w_value, preferred_element_type=jnp.float32).astype(jnp.bfloat16).reshape(seq_len, KV_HEADS, VALUE_DIM)
    group_size = HEADS // KV_HEADS
    query_rows = min(1024, seq_len)
    block_count = seq_len // query_rows
    key_pos = jnp.arange(seq_len, dtype=jnp.int32)

    def one_block(indices):
        head_idx, block_idx = indices
        kv_idx = head_idx // group_size
        row_first = block_idx * query_rows
        query_blk = lax.dynamic_slice(queries, (row_first, head_idx, jnp.int32(0), jnp.int32(0)), (query_rows, 1, 2, HEAD_DIM))[:, 0]
        key_head = lax.dynamic_index_in_dim(key_heads, kv_idx, 1, keepdims=False)
        value_head = lax.dynamic_index_in_dim(value_heads, kv_idx, 1, keepdims=False)
        query_pos = row_first + jnp.arange(query_rows, dtype=jnp.int32)
        visible = key_pos[None, :] <= query_pos[:, None]
        outputs = []
        log_list = []
        for map_idx in range(2):
            scores = jnp.dot(query_blk[:, map_idx], key_head[:, map_idx].T, preferred_element_type=jnp.float32) * HEAD_DIM ** (-0.5)
            scores = jnp.where(visible, scores, -jnp.inf)
            row_max = lax.optimization_barrier(jnp.max(scores, axis=1, keepdims=True))
            weights = jnp.exp(scores - row_max)
            row_total = lax.optimization_barrier(jnp.sum(weights, axis=1, keepdims=True))
            mixed_map = jnp.dot(weights.astype(jnp.bfloat16), value_head, preferred_element_type=jnp.float32) / row_total
            outputs.append(mixed_map)
            log_list.append((row_max + jnp.log(row_total))[:, 0])
        lam_value = lam_head[head_idx]
        diff_out = outputs[0] - lam_value * outputs[1]
        head_out = rms_scale(diff_out, sub_gain, 1e-06).astype(jnp.bfloat16)
        return (head_out, jnp.stack(log_list))
    head_ids = jnp.repeat(jnp.arange(HEADS, dtype=jnp.int32), block_count)
    block_ids = jnp.tile(jnp.arange(block_count, dtype=jnp.int32), HEADS)
    attn_blocks, lse_blocks = lax.map(one_block, (head_ids, block_ids))
    attn_out = attn_blocks.reshape(HEADS, block_count, query_rows, VALUE_DIM).transpose(1, 2, 0, 3).reshape(seq_len, HEADS * VALUE_DIM)
    log_sums = lse_blocks.reshape(HEADS, block_count, 2, query_rows).transpose(2, 0, 1, 3).reshape(2, HEADS, seq_len)
    conv_part = CONV_CH // N_TP
    attn_part = HEADS * VALUE_DIM // N_TP
    mixed_sum = jnp.zeros((seq_len, D), jnp.float32)
    for group_idx in range(N_TP):
        conv_lo = group_idx * conv_part
        attn_lo = group_idx * attn_part
        partial_value = jnp.dot(conv_out[:, conv_lo:conv_lo + conv_part], w_out_conv[conv_lo:conv_lo + conv_part], preferred_element_type=jnp.float32)
        partial_value = partial_value + jnp.dot(attn_out[:, attn_lo:attn_lo + attn_part], w_out_attn[attn_lo:attn_lo + attn_part], preferred_element_type=jnp.float32)
        mixed_sum = mixed_sum + lax.optimization_barrier(partial_value.astype(jnp.bfloat16)).astype(jnp.float32)
    return (mixed_sum.astype(jnp.bfloat16), log_sums)
```

```python
import functools

import jax
import jax.numpy as jnp
from jax import lax
from jax.experimental import pallas as pl
from jax.experimental.pallas import tpu as pltpu
from jax.sharding import PartitionSpec as P

KW = 31
MESH = pl.DeviceIdType.MESH
NZ, NX, NT = 8, 4, 4
BF, F32 = jnp.bfloat16, jnp.float32
VM = pl.BlockSpec(memory_space=pltpu.VMEM)
ANY = pl.BlockSpec(memory_space=pl.ANY)


def remote(src, dst, send, recv, device):
    return pltpu.make_async_remote_copy(
        src_ref=src, dst_ref=dst, send_sem=send, recv_sem=recv, device_id=device, device_id_type=MESH
    )


def greet(devices):
    barrier = pltpu.get_barrier_semaphore()
    for device in devices:
        pl.semaphore_signal(barrier, inc=1, device_id=device, device_id_type=MESH)
    return lambda: pl.semaphore_wait(barrier, len(devices))


def half_norm(value, gain):
    low = lax.broadcasted_iota(jnp.int32, value.shape, 1) < 64
    squares = value * value
    first = jnp.sum(jnp.where(low, squares, 0.0), axis=1, keepdims=True)
    second = jnp.sum(jnp.where(low, 0.0, squares), axis=1, keepdims=True)
    scale = jnp.where(low, lax.rsqrt(first / 64 + 1e-6), lax.rsqrt(second / 64 + 1e-6))
    return (value * scale * gain).astype(BF)


def front_kernel(
    tok, gain, wa_h, wb_h, wq_h, wk_h, wv_h, qg, kg,
    gated, q_own, q_far, kv,
    rows, normed, wa, wb, wq, wk, wv, w_sem, own_sem, s1, r1, s2, r2,
):
    y = lax.axis_index("tp")
    up, down = lax.rem(y + 1, NT), lax.rem(y + 3, NT)
    meet = greet([{"tp": up}, {"tp": down}])
    loads = [
        pltpu.make_async_copy(src, dst, w_sem.at[i])
        for i, (src, dst) in enumerate(((wa_h, wa), (wb_h, wb), (wq_h, wq), (wk_h, wk), (wv_h, wv)))
    ]
    own = pltpu.make_async_copy(tok, rows.at[y], own_sem)
    own.start()
    meet()
    sends = []

    def piece(slot, half):
        return rows.at[slot, pl.ds(half * 32, 32)]

    for order in range(2):
        for d, target in enumerate((up, down)):
            half = order if d == 0 else 1 - order
            copy = remote(tok.at[pl.ds(half * 32, 32)], piece(y, half), s1.at[d, half], r1.at[d, half], {"tp": target})
            copy.start()
            sends.append(copy)
    for load in loads:
        load.start()
    own.wait()

    def norm_slot(slot):
        value = rows[slot].astype(F32)
        scale = lax.rsqrt(jnp.mean(value * value, axis=1, keepdims=True) + 1e-6)
        normed[pl.ds(pl.multiple_of(slot * 64, 64), 64), :] = (value * scale * gain[...]).astype(BF)

    norm_slot(y)
    for d, (target, source) in enumerate(((up, down), (down, up))):
        half = d
        remote(piece(source, half), piece(source, half), s1.at[d, half], r1.at[d, half], {"tp": target}).wait_recv()
        copy = remote(piece(source, half), piece(source, half), s2.at[d], r2.at[d], {"tp": target})
        copy.start()
        sends.append(copy)
    for d, (target, source) in enumerate(((up, down), (down, up))):
        half = 1 - d
        remote(piece(source, half), piece(source, half), s1.at[d, half], r1.at[d, half], {"tp": target}).wait_recv()
        norm_slot(source)
    far = lax.rem(y + 2, NT)
    for d, target in enumerate((up, down)):
        remote(piece(far, d), piece(far, d), s2.at[d], r2.at[d], {"tp": target}).wait_recv()
    norm_slot(far)
    for load in loads:
        load.wait()
    value = normed[...]

    def dot(weight):
        return jnp.dot(value, weight, preferred_element_type=F32)

    key_value = dot(jnp.concatenate([wk[...], wv[...]], axis=1))
    keys = half_norm(key_value[:, :128], kg[...])
    for h in range(2):
        kv[h, :, 0:128] = keys[h * 128 : (h + 1) * 128].T
        kv[h, :, 128:256] = key_value[h * 128 : (h + 1) * 128, 128:].astype(BF)
    for n in range(2):
        span = slice(n * 256, (n + 1) * 256)
        queries = dot(wq[:, span])
        target = q_own if n == 0 else q_far
        for k in range(2):
            part = half_norm(queries[:, k * 128 : (k + 1) * 128], qg[2 * n + k : 2 * n + k + 1, :])
            target[:, k * 128 : (k + 1) * 128] = part * jnp.asarray(0.125, BF)
    for n in range(2):
        span = slice(n * 256, (n + 1) * 256)
        gated[:, span] = (dot(wa[:, span]) * jax.nn.sigmoid(dot(wb[:, span]))).astype(BF)
    for copy in sends:
        copy.wait_send()


def front(tokens, norm_gain, wa, wb, wq, wk, wv, query_gain, key_gain):
    dma = pltpu.SemaphoreType.DMA
    return pl.pallas_call(
        front_kernel,
        out_shape=(
            jax.ShapeDtypeStruct((256, 512), BF),
            jax.ShapeDtypeStruct((256, 256), BF),
            jax.ShapeDtypeStruct((256, 256), BF),
            jax.ShapeDtypeStruct((2, 128, 256), BF),
        ),
        in_specs=[VM, VM, ANY, ANY, ANY, ANY, ANY, VM, VM],
        out_specs=(VM, VM, VM, VM),
        scratch_shapes=[
            pltpu.VMEM((4, 64, 2048), BF),
            pltpu.VMEM((256, 2048), BF),
            pltpu.VMEM((2048, 512), BF),
            pltpu.VMEM((2048, 512), BF),
            pltpu.VMEM((2048, 512), BF),
            pltpu.VMEM((2048, 128), BF),
            pltpu.VMEM((2048, 128), BF),
            dma((5,)), dma, dma((2, 2)), dma((2, 2)), dma((2,)), dma((2,)),
        ],
        compiler_params=pltpu.CompilerParams(
            collective_id=0, has_side_effects=True, vmem_limit_bytes=40 * 1024 * 1024
        ),
        name="front",
    )(tokens, norm_gain.reshape(1, -1), wa, wb, wq, wk, wv, query_gain, key_gain)


def middle_kernel(
    kv_in, q_own, q_far, gated, taps, ln_gain, lam, sub_gain,
    attn, conv_out, logs,
    kv, q_in, qpad, m_ref, l_ref, acc, halo, gpad, csum, stat_out, stat_in, ret_out, ret_in, log_out, log_in, log_self,
    lc, ax_s, ax_r, az_s, az_r, bz_s, bz_r, bx_s, bx_r, dd_s, dd_r, ex_s, ex_r, st_s, st_r,
):
    sp, y = lax.axis_index("sp"), lax.axis_index("tp")
    z, x, c = sp // 8, lax.rem(sp // 2, 4), lax.rem(sp, 2)
    sib = 1 - c

    def zm(value):
        return lax.rem(value + 2 * NZ, NZ)

    def xm(value):
        return lax.rem(value + 2 * NX, NX)

    def at(zz, xx, cc):
        return {"sp": zz * 8 + xx * 2 + cc, "tp": y}

    zdev = (at(zm(z + 1), x, c), at(zm(z - 1), x, c))
    xdev = (at(z, xm(x + 1), c), at(z, xm(x - 1), c))
    sdev = at(z, x, sib)
    far_z = NZ - 1 - z
    pdev = at(far_z, x, c)
    nxt = {"sp": lax.rem(sp + 1, 64), "tp": y}
    prv = {"sp": lax.rem(sp + 63, 64), "tp": y}
    ydev = [{"sp": sp, "tp": lax.rem(y + k, NT)} for k in (1, 2, 3)]
    meet = greet([*zdev, *xdev, sdev, pdev, nxt, prv, *ydev])
    sends = []

    def go(copy):
        copy.start()
        sends.append(copy)

    def origin(s, d):
        return zm(z - s) if d == 0 else zm(z + s)

    def signs(s):
        return (0, 1) if 0 < s < 4 else (0,)

    def hop_halves(s, d):
        return (0, 1) if s < 4 else (d,)

    def ax1(d):
        ox = x if d is None else xm(x - 1 + 2 * d)
        return kv.at[c, 0, ox, z]

    def az(s, d, xh, landing):
        return kv.at[c, 0, pl.ds(xh * 2, 2), origin(s if landing else s - 1, d)]

    def bz(s, d, rh, landing):
        return kv.at[c, 1, x, origin(s if landing else s - 1, d), pl.ds(rh * 64, 64)]

    def az_send(s):
        for d in range(2):
            for xh in hop_halves(s, d):
                ref = az(s, d, xh, False)
                go(remote(ref, ref, az_s.at[s - 1, d, xh], az_r.at[s - 1, d, xh], zdev[d]))

    def az_recv(s):
        for d in range(2):
            for xh in hop_halves(s, d):
                ref = az(s, d, xh, True)
                remote(ref, ref, az_s.at[s - 1, d, xh], az_r.at[s - 1, d, xh], zdev[d]).wait_recv()

    def bz_send(s):
        for d in range(2):
            for rh in hop_halves(s, d):
                ref = bz(s, d, rh, False)
                src = kv_in.at[1, pl.ds(rh * 64, 64)] if s == 1 else ref
                go(remote(src, ref, bz_s.at[s - 1, d, rh], bz_r.at[s - 1, d, rh], zdev[d]))

    def bz_recv(s):
        for d in range(2):
            for rh in hop_halves(s, d):
                ref = bz(s, d, rh, True)
                remote(ref, ref, bz_s.at[s - 1, d, rh], bz_r.at[s - 1, d, rh], zdev[d]).wait_recv()

    def bx1_send(s):
        for g in signs(s):
            ref = kv.at[c, 1, x, origin(s, g)]
            for d in range(2):
                go(remote(kv_in.at[1] if s == 0 else ref, ref, bx_s.at[0, s, g, d], bx_r.at[0, s, g, d], xdev[d]))

    def bx1_recv(s):
        for g in signs(s):
            for d in range(2):
                ref = kv.at[c, 1, xm(x - 1 + 2 * d), origin(s, g)]
                remote(ref, ref, bx_s.at[0, s, g, d], bx_r.at[0, s, g, d], xdev[d]).wait_recv()

    def bx2_send(s):
        for g in signs(s):
            for d in range(2):
                ref = kv.at[c, 1, xm(x - 1 + 2 * d), origin(s, g), pl.ds(d * 64, 64)]
                go(remote(ref, ref, bx_s.at[1, s, g, d], bx_r.at[1, s, g, d], xdev[d]))

    def bx2_recv(s):
        for g in signs(s):
            for d in range(2):
                ref = kv.at[c, 1, xm(x + 2), origin(s, g), pl.ds(d * 64, 64)]
                remote(ref, ref, bx_s.at[1, s, g, d], bx_r.at[1, s, g, d], xdev[d]).wait_recv()

    def dd_send(h, s):
        for g in signs(s):
            ref = kv.at[c, h, :, origin(s, g)]
            go(remote(ref, ref, dd_s.at[h, s, g], dd_r.at[h, s, g], sdev))

    def dd_recv(h, s):
        for g in signs(s):
            ref = kv.at[sib, h, :, origin(s, g)]
            remote(ref, ref, dd_s.at[h, s, g], dd_r.at[h, s, g], sdev).wait_recv()

    def tile(which, cc, hh, zt, masked):
        keys = jnp.concatenate([kv[cc, hh, k, zt, :, 0:128] for k in range(NX)], axis=1)
        values = jnp.concatenate([kv[cc, hh, k, zt, :, 128:256] for k in range(NX)], axis=0)
        if masked:
            row = lax.broadcasted_iota(jnp.int32, (256, 128), 0) + (x * 512 + c * 256)
            col = lax.broadcasted_iota(jnp.int32, (256, 128), 1) + (cc * 256 + hh * 128)
        for hm in range(4):
            scores = jnp.dot(qpad[which, hm], keys, preferred_element_type=F32)
            parts = [scores[:, k * 128 : (k + 1) * 128] for k in range(NX)]
            if masked:
                parts = [jnp.where(col + k * 512 <= row, part, -1e30) for k, part in enumerate(parts)]
            top = jnp.maximum(jnp.maximum(parts[0], parts[1]), jnp.maximum(parts[2], parts[3]))
            old = m_ref[which, hm]
            new = jnp.maximum(old, jnp.max(top, axis=1, keepdims=True))
            fade = jnp.exp(old - new)
            parts = [jnp.exp(part - new) for part in parts]
            m_ref[which, hm] = new
            l_ref[which, hm] = l_ref[which, hm] * fade + ((parts[0] + parts[1]) + (parts[2] + parts[3]))
            weights = jnp.concatenate([part.astype(BF) for part in parts], axis=1)
            acc[which, hm] = acc[which, hm] * fade + jnp.dot(weights, values, preferred_element_type=F32)

    def attend(s):
        def step(i, carry):
            which = lax.rem(i, 2)
            hh = lax.rem(i // 2, 2)
            cc = lax.rem(i // 4, 2)
            g = i // 8
            zt = zm(z - s + 2 * s * g)
            zq = jnp.where(which == 0, z, far_z)

            @pl.when(zt < zq)
            def _():
                tile(which, cc, hh, zt, False)

            if s in (0, 1, 3):

                @pl.when(zt == zq)
                def _():
                    tile(which, cc, hh, zt, True)

            return carry

        lax.fori_loop(0, 8 * len(signs(s)), step, 0)

    def stage(e):
        if 1 <= e <= 4:
            bz_recv(e)
            if e < 4:
                bz_send(e + 1)
            bx1_send(e)
        if 0 <= e - 1 <= 4:
            bx1_recv(e - 1)
            bx2_send(e - 1)
        if e == 1:
            for d in range(2):
                ref = ax1(d)
                remote(ref, ref, ax_s.at[0, d], ax_r.at[0, d], xdev[d]).wait_recv()
                ref = kv.at[c, 0, xm(x - 1 + 2 * d), z, pl.ds(d * 64, 64)]
                go(remote(ref, ref, ax_s.at[1, d], ax_r.at[1, d], xdev[d]))
        if e == 2:
            for d in range(2):
                ref = kv.at[c, 0, xm(x + 2), z, pl.ds(d * 64, 64)]
                remote(ref, ref, ax_s.at[1, d], ax_r.at[1, d], xdev[d]).wait_recv()
            az_send(1)
            dd_send(0, 0)
        if 0 <= e - 2 <= 4:
            bx2_recv(e - 2)
            dd_send(1, e - 2)
        if 3 <= e <= 6:
            az_recv(e - 2)
            if e < 6:
                az_send(e - 1)
            dd_send(0, e - 2)
        if e >= 3:
            dd_recv(0, e - 3)
            dd_recv(1, e - 3)
            attend(e - 3)

    own = [pltpu.make_async_copy(kv_in.at[h], kv.at[c, h, x, z], lc.at[h]) for h in range(2)]
    for copy in own:
        copy.start()
    meet()
    for d in range(2):
        go(remote(kv_in.at[0], ax1(None), ax_s.at[0, d], ax_r.at[0, d], xdev[d]))
    bz_send(1)
    bx1_send(0)
    q_copy = remote(q_far, q_in, ex_s.at[0], ex_r.at[0], pdev)
    go(q_copy)
    halo_copy = remote(gated.at[pl.ds(224, 32)], halo, ex_s.at[1], ex_r.at[1], nxt)
    go(halo_copy)
    for copy in own:
        copy.wait()

    m_ref[...] = jnp.full(m_ref.shape, -1e30, F32)
    l_ref[...] = jnp.zeros(l_ref.shape, F32)
    acc[...] = jnp.zeros(acc.shape, F32)
    low = lax.broadcasted_iota(jnp.int32, (256, 128), 1) < 64

    def pad(which, source):
        for k in range(2):
            head = source[:, k * 128 : (k + 1) * 128].astype(F32)
            qpad[which, 2 * k] = jnp.where(low, head, 0.0).astype(BF)
            qpad[which, 2 * k + 1] = jnp.where(low, 0.0, head).astype(BF)

    pad(0, q_own)
    for k in range(4):
        gpad[k, 32:288, :] = gated[:, k * 128 : (k + 1) * 128].astype(F32)
    stage(1)
    halo_copy.wait_recv()
    for k in range(4):
        gpad[k, 0:32, :] = jnp.where(sp > 0, halo[:, k * 128 : (k + 1) * 128].astype(F32), 0.0)
    q_copy.wait_recv()
    pad(1, q_in)

    def conv_step(k, carry):
        one, two = carry
        total = jnp.zeros((256, 128), F32)
        for j in range(KW):
            total = total + taps[k, j : j + 1, :] * gpad[k, j + 2 : j + 258, :]
        csum[k] = total
        return one + total, two + total * total

    nothing = jnp.zeros((256, 128), F32)
    one, two = lax.fori_loop(0, 4, conv_step, (nothing, nothing))
    lane = lax.broadcasted_iota(jnp.int32, (256, 128), 1)
    stat_out[...] = jnp.where(
        lane == 0, jnp.sum(one, axis=1, keepdims=True), jnp.sum(two, axis=1, keepdims=True)
    )
    for k in range(3):
        go(remote(stat_out, stat_in.at[k], st_s.at[k], st_r.at[k], ydev[k]))
    stage(2)
    for k in range(3):
        remote(stat_out, stat_in.at[k], st_s.at[k], st_r.at[k], ydev[k]).wait_recv()
    total = (stat_out[...] + stat_in[0]) + (stat_in[1] + stat_in[2])
    mean = total[:, 0:1] / (NT * 512)
    mean_sq = total[:, 1:2] / (NT * 512)
    scale = lax.rsqrt(mean_sq - mean * mean + 1e-5)
    for k in range(4):
        span = slice(k * 128, (k + 1) * 128)
        conv_out[:, span] = jax.nn.silu((csum[k] - mean) * scale * ln_gain[:, span]).astype(BF)

    for e in range(3, 8):
        stage(e)

    def finish(which, out_ref, log_ref):
        table = jnp.zeros((256, 128), F32)
        for k in range(2):
            outs = []
            for m in range(2):
                total = jnp.sum(l_ref[which, 2 * k + m], axis=1, keepdims=True)
                outs.append(acc[which, 2 * k + m] / total)
                table = jnp.where(lane == 2 * k + m, m_ref[which, 2 * k + m] + jnp.log(total), table)
            row = 2 * which + k
            diff = outs[0] - lam[row : row + 1, :] * outs[1]
            scale = lax.rsqrt(jnp.mean(diff * diff, axis=1, keepdims=True) + 1e-6)
            out_ref[:, k * 128 : (k + 1) * 128] = (diff * scale * sub_gain[...]).astype(BF)
        log_ref[...] = table.T[0:8, :]

    finish(1, ret_out, log_out)
    back = [
        remote(ret_out, ret_in, ex_s.at[2], ex_r.at[2], pdev),
        remote(log_out, log_in, ex_s.at[3], ex_r.at[3], pdev),
    ]
    for copy in back:
        go(copy)
    finish(0, attn.at[:, pl.ds(0, 256)], log_self)
    for k in range(2):
        for m in range(2):
            logs[m, k : k + 1, :] = log_self[2 * k + m : 2 * k + m + 1, :]
    for copy in back:
        copy.wait_recv()
    attn[:, 256:512] = ret_in[...]
    for k in range(2):
        for m in range(2):
            logs[m, 2 + k : 3 + k, :] = log_in[2 * k + m : 2 * k + m + 1, :]
    for copy in sends:
        copy.wait_send()


def middle(kv, q_own, q_far, gated, taps, ln_gain, lam_head, sub_gain):
    dma = pltpu.SemaphoreType.DMA
    taps = taps.reshape(KW, 4, 128).transpose(1, 0, 2)
    lam = jnp.broadcast_to(lam_head[:, None], (4, 128))
    return pl.pallas_call(
        middle_kernel,
        out_shape=(
            jax.ShapeDtypeStruct((256, 512), BF),
            jax.ShapeDtypeStruct((256, 512), BF),
            jax.ShapeDtypeStruct((2, 4, 256), F32),
        ),
        in_specs=[VM] * 8,
        out_specs=(VM, VM, VM),
        scratch_shapes=[
            pltpu.VMEM((2, 2, NX, NZ, 128, 256), BF),
            pltpu.VMEM((256, 256), BF),
            pltpu.VMEM((2, 4, 256, 128), BF),
            pltpu.VMEM((2, 4, 256, 128), F32),
            pltpu.VMEM((2, 4, 256, 128), F32),
            pltpu.VMEM((2, 4, 256, 128), F32),
            pltpu.VMEM((32, 512), BF),
            pltpu.VMEM((4, 288, 128), F32),
            pltpu.VMEM((4, 256, 128), F32),
            pltpu.VMEM((256, 128), F32),
            pltpu.VMEM((3, 256, 128), F32),
            pltpu.VMEM((256, 256), BF),
            pltpu.VMEM((256, 256), BF),
            pltpu.VMEM((8, 256), F32),
            pltpu.VMEM((8, 256), F32),
            pltpu.VMEM((8, 256), F32),
            dma((2,)),
            dma((2, 2)), dma((2, 2)),
            dma((4, 2, 2)), dma((4, 2, 2)),
            dma((4, 2, 2)), dma((4, 2, 2)),
            dma((2, 5, 2, 2)), dma((2, 5, 2, 2)),
            dma((2, 5, 2)), dma((2, 5, 2)),
            dma((4,)), dma((4,)),
            dma((3,)), dma((3,)),
        ],
        compiler_params=pltpu.CompilerParams(
            collective_id=1, has_side_effects=True, vmem_limit_bytes=44 * 1024 * 1024
        ),
        name="middle",
    )(kv, q_own, q_far, gated, taps, ln_gain.reshape(1, -1), lam, sub_gain.reshape(1, -1))


def back_kernel(conv, attn, w_conv, w_attn, mixed, part, far, near, total, r1, r2, s1, q1, s2, q2):
    y = lax.axis_index("tp")
    targets = ({"tp": lax.rem(y + 1, NT)}, {"tp": lax.rem(y + 3, NT)})
    meet = greet(targets)
    own = lax.rem(y + 4, NT)
    blocks = (lax.rem(y + 1, NT), lax.rem(y + 3, NT))
    opposite = lax.rem(y + 2, NT)
    sends = []

    def go(copy):
        copy.start()
        sends.append(copy)

    def rows(block):
        return pl.ds(pl.multiple_of(block * 64, 64), 64)

    for n in range(4):
        span = pl.ds(n * 512, 512)
        part[:, span] = jnp.dot(conv[...], w_conv[:, span], preferred_element_type=F32) + jnp.dot(
            attn[...], w_attn[:, span], preferred_element_type=F32
        )
        if n % 2 == 1:
            d = n // 2
            wide = pl.ds(d * 1024, 1024)
            far[d] = part[rows(opposite), wide].astype(BF)
            near[d] = part[rows(blocks[1 - d]), wide].astype(BF)
            if d == 0:
                meet()
            go(remote(far.at[d], r1.at[d], s1.at[d], q1.at[d], targets[d]))
            go(remote(near.at[d], r2.at[1 - d, d], s2.at[1 - d, d], q2.at[1 - d, d], targets[1 - d]))
    for d in range(2):
        remote(far.at[d], r1.at[d], s1.at[d], q1.at[d], targets[d]).wait_recv()
        wide = pl.ds(d * 1024, 1024)
        total[d] = (part[rows(blocks[d]), wide] + r1[d].astype(F32)).astype(BF)
        go(remote(total.at[d], r2.at[d, d], s2.at[d, d], q2.at[d, d], targets[d]))
    for d in (1, 0):
        for k in (1 - d, d):
            remote(total.at[d], r2.at[k, d], s2.at[k, d], q2.at[k, d], targets[k]).wait_recv()
        wide = pl.ds(d * 1024, 1024)
        mixed[:, wide] = (part[rows(own), wide] + (r2[0, d].astype(F32) + r2[1, d].astype(F32))).astype(BF)
    for copy in sends:
        copy.wait_send()


def back(conv, attn, w_conv, w_attn):
    dma = pltpu.SemaphoreType.DMA
    return pl.pallas_call(
        back_kernel,
        out_shape=jax.ShapeDtypeStruct((64, 2048), BF),
        in_specs=[VM] * 4,
        out_specs=VM,
        scratch_shapes=[
            pltpu.VMEM((256, 2048), F32),
            pltpu.VMEM((2, 64, 1024), BF),
            pltpu.VMEM((2, 64, 1024), BF),
            pltpu.VMEM((2, 64, 1024), BF),
            pltpu.VMEM((2, 64, 1024), BF),
            pltpu.VMEM((2, 2, 64, 1024), BF),
            dma((2,)), dma((2,)), dma((2, 2)), dma((2, 2)),
        ],
        compiler_params=pltpu.CompilerParams(
            collective_id=2, has_side_effects=True, vmem_limit_bytes=24 * 1024 * 1024
        ),
        name="back",
    )(conv, attn, w_conv, w_attn)


def on_device(
    tokens, norm_gain, w_glu_a, w_glu_b, conv_taps, ln_gain, w_query, w_key, w_value,
    query_gain, key_gain, lam_head, sub_gain, w_out_conv, w_out_attn,
):
    gated, q_own, q_far, kv = front(
        tokens, norm_gain, w_glu_a, w_glu_b, w_query, w_key, w_value, query_gain, key_gain
    )
    attn, conv_out, logs = middle(kv, q_own, q_far, gated, conv_taps, ln_gain, lam_head, sub_gain)
    return back(conv_out, attn, w_out_conv, w_out_attn), logs


def solution(mesh):
    return jax.shard_map(
        on_device,
        mesh=mesh,
        in_specs=(
            P(("sp", "tp"), None), P(), P(None, "tp"), P(None, "tp"), P(None, "tp"), P("tp"),
            P(None, "tp"), P(None, "tp"), P(None, "tp"), P("tp", None), P("tp", None), P("tp"),
            P(), P("tp", None), P("tp", None),
        ),
        out_specs=(P(("sp", "tp"), None), P(None, "tp", "sp")),
        check_vma=False,
    )
```

```python
import functools

import jax
import jax.numpy as jnp
from jax import lax
from jax.experimental import pallas as pl
from jax.experimental.pallas import tpu as pltpu
from jax.sharding import PartitionSpec as P

KW = 31
MESH = pl.DeviceIdType.MESH
NZ, NX, NT = 8, 4, 4
BF, F32 = jnp.bfloat16, jnp.float32
VM = pl.BlockSpec(memory_space=pltpu.VMEM)


def remote(src, dst, send, recv, device):
    return pltpu.make_async_remote_copy(
        src_ref=src, dst_ref=dst, send_sem=send, recv_sem=recv, device_id=device, device_id_type=MESH
    )


def greet(devices):
    barrier = pltpu.get_barrier_semaphore()
    for device in devices:
        pl.semaphore_signal(barrier, inc=1, device_id=device, device_id_type=MESH)
    return lambda: pl.semaphore_wait(barrier, len(devices))


def half_norm(value, gain):
    low = lax.broadcasted_iota(jnp.int32, value.shape, 1) < 64
    squares = value * value
    first = jnp.sum(jnp.where(low, squares, 0.0), axis=1, keepdims=True)
    second = jnp.sum(jnp.where(low, 0.0, squares), axis=1, keepdims=True)
    scale = jnp.where(low, lax.rsqrt(first / 64 + 1e-6), lax.rsqrt(second / 64 + 1e-6))
    return (value * scale * gain).astype(BF)


HBM = pl.BlockSpec(memory_space=pltpu.MemorySpace.HBM)
SM = pl.BlockSpec(memory_space=pltpu.SMEM)


def layer_kernel(
    tok, gain, wa_h, wb_h, wq_h, wk_h, wv_h, qg, kg, taps, ln_gain, lam, sub_gain, wc_h, wo_h,
    mixed, logs,
    rows, normed, wa, wb, wq, wk, wv, wc, wo, gated, kv_in, q_own, q_far,
    kv, q_in, qpad, m_ref, l_ref, acc, halo, gpad, csum, stat_out, stat_in,
    attn, conv_out, ret_out, ret_in, log_out, log_in, log_self,
    part, far, near, total_out, r1, r2,
    w_sem, own_sem, y1s, y1r, y2s, y2r,
    lc, ax_s, ax_r, az_s, az_r, bz_s, bz_r, bx_s, bx_r, dd_s, dd_r, ex_s, ex_r, st_s, st_r,
    o1s, o1r, o2s, o2r,
):
    sp, y = lax.axis_index("sp"), lax.axis_index("tp")
    z, x, c = sp // 8, lax.rem(sp // 2, 4), lax.rem(sp, 2)
    sib = 1 - c

    def zm(value):
        return lax.rem(value + 2 * NZ, NZ)

    def xm(value):
        return lax.rem(value + 2 * NX, NX)

    def at(zz, xx, cc):
        return {"sp": zz * 8 + xx * 2 + cc, "tp": y}

    zdev = (at(zm(z + 1), x, c), at(zm(z - 1), x, c))
    xdev = (at(z, xm(x + 1), c), at(z, xm(x - 1), c))
    sdev = at(z, x, sib)
    far_z = NZ - 1 - z
    pdev = at(far_z, x, c)
    nxt = {"sp": lax.rem(sp + 1, 64), "tp": y}
    prv = {"sp": lax.rem(sp + 63, 64), "tp": y}
    ydev = [{"sp": sp, "tp": lax.rem(y + k, NT)} for k in (1, 2, 3)]
    up, down = ydev[0], ydev[2]
    meet = greet([*zdev, *xdev, sdev, pdev, nxt, prv, *ydev])
    sends = []

    def go(copy):
        copy.start()
        sends.append(copy)

    def origin(s, d):
        return zm(z - s) if d == 0 else zm(z + s)

    def signs(s):
        return (0, 1) if 0 < s < 4 else (0,)

    def hop_halves(s, d):
        return (0, 1) if s < 4 else (d,)

    def ax1(d):
        ox = x if d is None else xm(x - 1 + 2 * d)
        return kv.at[c, 0, ox, z]

    def az(s, d, xh, landing):
        return kv.at[c, 0, pl.ds(xh * 2, 2), origin(s if landing else s - 1, d)]

    def bz(s, d, rh, landing):
        return kv.at[c, 1, x, origin(s if landing else s - 1, d), pl.ds(rh * 64, 64)]

    def az_send(s, xh):
        for d in range(2):
            if xh in hop_halves(s, d):
                ref = az(s, d, xh, False)
                go(remote(ref, ref, az_s.at[s - 1, d, xh], az_r.at[s - 1, d, xh], zdev[d]))

    def az_recv(s, xh):
        for d in range(2):
            if xh in hop_halves(s, d):
                ref = az(s, d, xh, True)
                remote(ref, ref, az_s.at[s - 1, d, xh], az_r.at[s - 1, d, xh], zdev[d]).wait_recv()

    def bz_send(s):
        for d in range(2):
            for rh in hop_halves(s, d):
                ref = bz(s, d, rh, False)
                src = kv_in.at[1, pl.ds(rh * 64, 64)] if s == 1 else ref
                go(remote(src, ref, bz_s.at[s - 1, d, rh], bz_r.at[s - 1, d, rh], zdev[d]))

    def bz_recv(s):
        for d in range(2):
            for rh in hop_halves(s, d):
                ref = bz(s, d, rh, True)
                remote(ref, ref, bz_s.at[s - 1, d, rh], bz_r.at[s - 1, d, rh], zdev[d]).wait_recv()

    def bx1_send(s):
        for g in signs(s):
            ref = kv.at[c, 1, x, origin(s, g)]
            for d in range(2):
                go(remote(kv_in.at[1] if s == 0 else ref, ref, bx_s.at[0, s, g, d], bx_r.at[0, s, g, d], xdev[d]))

    def bx1_recv(s):
        for g in signs(s):
            for d in range(2):
                ref = kv.at[c, 1, xm(x - 1 + 2 * d), origin(s, g)]
                remote(ref, ref, bx_s.at[0, s, g, d], bx_r.at[0, s, g, d], xdev[d]).wait_recv()

    def bx2_send(s):
        for g in signs(s):
            for d in range(2):
                ref = kv.at[c, 1, xm(x - 1 + 2 * d), origin(s, g), pl.ds(d * 64, 64)]
                go(remote(ref, ref, bx_s.at[1, s, g, d], bx_r.at[1, s, g, d], xdev[d]))

    def bx2_recv(s):
        for g in signs(s):
            for d in range(2):
                ref = kv.at[c, 1, xm(x + 2), origin(s, g), pl.ds(d * 64, 64)]
                remote(ref, ref, bx_s.at[1, s, g, d], bx_r.at[1, s, g, d], xdev[d]).wait_recv()

    def dd_send(h, s):
        for g in signs(s):
            ref = kv.at[c, h, :, origin(s, g)]
            go(remote(ref, ref, dd_s.at[h, s, g], dd_r.at[h, s, g], sdev))

    def dd_recv(h, s):
        for g in signs(s):
            ref = kv.at[sib, h, :, origin(s, g)]
            remote(ref, ref, dd_s.at[h, s, g], dd_r.at[h, s, g], sdev).wait_recv()

    def tile(which, cc, zt, masked):
        pieces = [(h, k) for h in range(2) for k in range(NX)]
        keys = jnp.concatenate([kv[cc, h, k, zt, :, 0:128] for h, k in pieces], axis=1)
        values = jnp.concatenate([kv[cc, h, k, zt, :, 128:256] for h, k in pieces], axis=0)
        if masked:
            row = lax.broadcasted_iota(jnp.int32, (256, 128), 0) + (x * 512 + c * 256)
            col = lax.broadcasted_iota(jnp.int32, (256, 128), 1) + cc * 256
        scores = jnp.dot(qpad[which].reshape(1024, 128), keys, preferred_element_type=F32)
        weights, fades = [], []
        for hm in range(4):
            parts = [scores[hm * 256 : (hm + 1) * 256, k * 128 : (k + 1) * 128] for k in range(8)]
            if masked:
                parts = [
                    jnp.where(col + (h * 128 + k * 512) <= row, item, -1e30)
                    for item, (h, k) in zip(parts, pieces)
                ]
            old = m_ref[which, hm]
            new = jnp.maximum(old, jnp.max(functools.reduce(jnp.maximum, parts), axis=1, keepdims=True))
            fade = jnp.exp(old - new)
            parts = [jnp.exp(item - new) for item in parts]
            m_ref[which, hm] = new
            l_ref[which, hm] = l_ref[which, hm] * fade + functools.reduce(jnp.add, parts)
            weights.append(jnp.concatenate([item.astype(BF) for item in parts], axis=1))
            fades.append(fade)
        outs = jnp.dot(jnp.concatenate(weights, axis=0), values, preferred_element_type=F32)
        for hm in range(4):
            acc[which, hm] = acc[which, hm] * fades[hm] + outs[hm * 256 : (hm + 1) * 256]

    def attend(s, g, cores):
        zt = zm(z - s + 2 * s * g)

        def step(i, carry):
            which = lax.rem(i, 2)
            cc = lax.rem(c + i // 2, 2)
            zq = jnp.where(which == 0, z, far_z)

            @pl.when(zt < zq)
            def _():
                tile(which, cc, zt, False)

            if s in (0, 1, 3):

                @pl.when(zt == zq)
                def _():
                    tile(which, cc, zt, True)

            return carry

        lax.fori_loop(2 * cores[0], 2 * cores[1], step, 0)

    def stage(e):
        if 1 <= e <= 4:
            bz_recv(e)
            if e < 4:
                bz_send(e + 1)
            bx1_send(e)
        if 0 <= e - 1 <= 4:
            bx1_recv(e - 1)
            bx2_send(e - 1)
        if e == 1:
            for d in range(2):
                ref = ax1(d)
                remote(ref, ref, ax_s.at[0, d], ax_r.at[0, d], xdev[d]).wait_recv()
                ref = kv.at[c, 0, xm(x - 1 + 2 * d), z, pl.ds(d * 64, 64)]
                go(remote(ref, ref, ax_s.at[1, d], ax_r.at[1, d], xdev[d]))
        if e == 2:
            for d in range(2):
                ref = kv.at[c, 0, xm(x + 2), z, pl.ds(d * 64, 64)]
                remote(ref, ref, ax_s.at[1, d], ax_r.at[1, d], xdev[d]).wait_recv()
            az_send(1, 0)
            az_send(1, 1)
            dd_send(0, 0)
        if 0 <= e - 2 <= 4:
            bx2_recv(e - 2)
            dd_send(1, e - 2)
        if e == 3:
            attend(0, 0, (0, 1))
        for xh in range(2):
            if 3 <= e <= 6:
                az_recv(e - 2, xh)
                if e < 6:
                    az_send(e - 1, xh)
            if e > 3 and xh == 0:
                dd_recv(0, e - 3)
                dd_recv(1, e - 3)
                attend(e - 3, 0, (0, 2))
        if 3 <= e <= 6:
            dd_send(0, e - 2)
        if e == 3:
            dd_recv(0, 0)
            dd_recv(1, 0)
            attend(0, 0, (1, 2))
        elif 3 < e < 7:
            attend(e - 3, 1, (0, 2))

    pairs = ((wk_h, wk), (wv_h, wv), (wq_h, wq), (wa_h, wa), (wb_h, wb), (wc_h, wc), (wo_h, wo))
    loads = [pltpu.make_async_copy(src, dst, w_sem.at[i]) for i, (src, dst) in enumerate(pairs)]
    own_rows = pltpu.make_async_copy(tok, rows.at[y], own_sem)
    own_rows.start()
    meet()

    def piece(slot, half):
        return rows.at[slot, pl.ds(half * 32, 32)]

    ypair = ((up, lax.rem(y + 3, NT)), (down, lax.rem(y + 1, NT)))
    for order in range(2):
        for d in range(2):
            half = order if d == 0 else 1 - order
            go(remote(tok.at[pl.ds(half * 32, 32)], piece(y, half), y1s.at[d, half], y1r.at[d, half], ypair[d][0]))
    for load in loads:
        load.start()
    own_rows.wait()

    def norm_slot(slot):
        value = rows[slot].astype(F32)
        scale = lax.rsqrt(jnp.mean(value * value, axis=1, keepdims=True) + 1e-6)
        normed[pl.ds(pl.multiple_of(slot * 64, 64), 64), :] = (value * scale * gain[...]).astype(BF)

    norm_slot(y)
    m_ref[...] = jnp.full(m_ref.shape, -1e30, F32)
    l_ref[...] = jnp.zeros(l_ref.shape, F32)
    acc[...] = jnp.zeros(acc.shape, F32)
    for d in range(2):
        target, source = ypair[d]
        ref = piece(source, d)
        remote(ref, ref, y1s.at[d, d], y1r.at[d, d], target).wait_recv()
        go(remote(ref, ref, y2s.at[d], y2r.at[d], target))
    for d in range(2):
        target, source = ypair[d]
        ref = piece(source, 1 - d)
        remote(ref, ref, y1s.at[d, 1 - d], y1r.at[d, 1 - d], target).wait_recv()
        norm_slot(source)
    opposite = lax.rem(y + 2, NT)
    for d in range(2):
        ref = piece(opposite, d)
        remote(ref, ref, y2s.at[d], y2r.at[d], ypair[d][0]).wait_recv()
    norm_slot(opposite)

    def dot(weight):
        return jnp.dot(normed[...], weight, preferred_element_type=F32)

    for load in loads[:3]:
        load.wait()
    key_value = dot(jnp.concatenate([wk[...], wv[...]], axis=1))
    keys_all = half_norm(key_value[:, :128], kg[...])
    for h in range(2):
        kv_in[h, :, 0:128] = keys_all[h * 128 : (h + 1) * 128].T
        kv_in[h, :, 128:256] = key_value[h * 128 : (h + 1) * 128, 128:].astype(BF)

    def project_q(n, target):
        queries = dot(wq[:, n * 256 : (n + 1) * 256])
        for k in range(2):
            one = half_norm(queries[:, k * 128 : (k + 1) * 128], qg[2 * n + k : 2 * n + k + 1, :])
            target[:, k * 128 : (k + 1) * 128] = one * jnp.asarray(0.125, BF)

    project_q(1, q_far)
    own = [pltpu.make_async_copy(kv_in.at[h], kv.at[c, h, x, z], lc.at[h]) for h in range(2)]
    for copy in own:
        copy.start()
    for d in range(2):
        go(remote(kv_in.at[0], ax1(None), ax_s.at[0, d], ax_r.at[0, d], xdev[d]))
    bz_send(1)
    bx1_send(0)
    for load in loads[3:5]:
        load.wait()
    for n in range(2):
        span = slice(n * 256, (n + 1) * 256)
        gated[:, span] = (dot(wa[:, span]) * jax.nn.sigmoid(dot(wb[:, span]))).astype(BF)
    q_copy = remote(q_far, q_in, ex_s.at[0], ex_r.at[0], pdev)
    go(q_copy)
    project_q(0, q_own)
    halo_copy = remote(gated.at[pl.ds(224, 32)], halo, ex_s.at[1], ex_r.at[1], nxt)
    go(halo_copy)
    for copy in own:
        copy.wait()
    stage(1)
    low = lax.broadcasted_iota(jnp.int32, (256, 128), 1) < 64

    def pad(which, source):
        for k in range(2):
            head = source[:, k * 128 : (k + 1) * 128].astype(F32)
            qpad[which, 2 * k] = jnp.where(low, head, 0.0).astype(BF)
            qpad[which, 2 * k + 1] = jnp.where(low, 0.0, head).astype(BF)

    pad(0, q_own)
    for k in range(4):
        gpad[k, 32:288, :] = gated[:, k * 128 : (k + 1) * 128].astype(F32)
    halo_copy.wait_recv()
    for k in range(4):
        gpad[k, 0:32, :] = jnp.where(sp > 0, halo[:, k * 128 : (k + 1) * 128].astype(F32), 0.0)

    def conv_step(k, carry):
        one, two = carry
        total = jnp.zeros((256, 128), F32)
        lanes = pl.ds(pl.multiple_of(k * 128, 128), 128)
        for j in range(KW):
            total = total + taps[j : j + 1, lanes] * gpad[k, j + 2 : j + 258, :]
        csum[k] = total
        return one + total, two + total * total

    nothing = jnp.zeros((256, 128), F32)
    one, two = lax.fori_loop(0, 2, conv_step, (nothing, nothing))
    stage(2)
    one, two = lax.fori_loop(2, 4, conv_step, (one, two))
    lane = lax.broadcasted_iota(jnp.int32, (256, 128), 1)
    stat_out[...] = jnp.where(
        lane == 0, jnp.sum(one, axis=1, keepdims=True), jnp.sum(two, axis=1, keepdims=True)
    )
    q_copy.wait_recv()
    pad(1, q_in)
    for k in range(3):
        go(remote(stat_out, stat_in.at[k], st_s.at[k], st_r.at[k], ydev[k]))
    stage(3)
    for k in range(3):
        remote(stat_out, stat_in.at[k], st_s.at[k], st_r.at[k], ydev[k]).wait_recv()
    total = (stat_out[...] + stat_in[0]) + (stat_in[1] + stat_in[2])
    mean = total[:, 0:1] / (NT * 512)
    mean_sq = total[:, 1:2] / (NT * 512)
    scale = lax.rsqrt(mean_sq - mean * mean + 1e-5)
    for k in range(4):
        span = slice(k * 128, (k + 1) * 128)
        conv_out[:, span] = jax.nn.silu((csum[k] - mean) * scale * ln_gain[:, span]).astype(BF)
    for load in loads[5:]:
        load.wait()
    for n in range(4):
        span = pl.ds(n * 512, 512)
        part[:, span] = jnp.dot(conv_out[...], wc[:, span], preferred_element_type=F32)

    for e in range(4, 8):
        stage(e)

    def finish(which, out_ref, log_ref):
        table = jnp.zeros((256, 128), F32)
        for k in range(2):
            outs = []
            for m in range(2):
                total = jnp.sum(l_ref[which, 2 * k + m], axis=1, keepdims=True)
                outs.append(acc[which, 2 * k + m] / total)
                table = jnp.where(lane == 2 * k + m, m_ref[which, 2 * k + m] + jnp.log(total), table)
            row = 2 * which + k
            diff = outs[0] - lam[row] * outs[1]
            scale = lax.rsqrt(jnp.mean(diff * diff, axis=1, keepdims=True) + 1e-6)
            out_ref[:, k * 128 : (k + 1) * 128] = (diff * scale * sub_gain[...]).astype(BF)
        log_ref[...] = table.T[0:8, :]

    finish(1, ret_out, log_out)
    back = [
        remote(ret_out, ret_in, ex_s.at[2], ex_r.at[2], pdev),
        remote(log_out, log_in, ex_s.at[3], ex_r.at[3], pdev),
    ]
    for copy in back:
        go(copy)
    finish(0, attn, log_self)
    for n in range(4):
        span = pl.ds(n * 512, 512)
        part[:, span] += jnp.dot(attn[...], wo[0:256, span], preferred_element_type=F32)
    for copy in back:
        copy.wait_recv()
    for which, table in ((0, log_self), (1, log_in)):
        for k in range(2):
            for m in range(2):
                logs[m, 2 * which + k : 2 * which + k + 1, :] = table[2 * k + m : 2 * k + m + 1, :]

    targets = (up, down)
    blocks = (lax.rem(y + 1, NT), lax.rem(y + 3, NT))

    def block_rows(block):
        return pl.ds(pl.multiple_of(block * 64, 64), 64)

    for n in range(4):
        span = pl.ds(n * 512, 512)
        part[:, span] += jnp.dot(ret_in[...], wo[256:512, span], preferred_element_type=F32)
        if n % 2 == 1:
            d = n // 2
            wide = pl.ds(d * 1024, 1024)
            far[d] = part[block_rows(opposite), wide].astype(BF)
            near[d] = part[block_rows(blocks[1 - d]), wide].astype(BF)
            go(remote(far.at[d], r1.at[d], o1s.at[d], o1r.at[d], targets[d]))
            go(remote(near.at[d], r2.at[1 - d, d], o2s.at[1 - d, d], o2r.at[1 - d, d], targets[1 - d]))
    for d in range(2):
        remote(far.at[d], r1.at[d], o1s.at[d], o1r.at[d], targets[d]).wait_recv()
        wide = pl.ds(d * 1024, 1024)
        total_out[d] = (part[block_rows(blocks[d]), wide] + r1[d].astype(F32)).astype(BF)
        go(remote(total_out.at[d], r2.at[d, d], o2s.at[d, d], o2r.at[d, d], targets[d]))
    for d in (1, 0):
        for k in (1 - d, d):
            remote(total_out.at[d], r2.at[k, d], o2s.at[k, d], o2r.at[k, d], targets[k]).wait_recv()
        wide = pl.ds(d * 1024, 1024)
        mixed[:, wide] = (part[block_rows(y), wide] + (r2[0, d].astype(F32) + r2[1, d].astype(F32))).astype(BF)
    for copy in sends:
        copy.wait_send()


def on_device(
    tokens, norm_gain, w_glu_a, w_glu_b, conv_taps, ln_gain, w_query, w_key, w_value,
    query_gain, key_gain, lam_head, sub_gain, w_out_conv, w_out_attn,
):
    dma = pltpu.SemaphoreType.DMA

    def vm(*shape, dtype=BF):
        return pltpu.VMEM(shape, dtype)

    return pl.pallas_call(
        layer_kernel,
        out_shape=(jax.ShapeDtypeStruct((64, 2048), BF), jax.ShapeDtypeStruct((2, 4, 256), F32)),
        in_specs=[VM, VM, HBM, HBM, HBM, HBM, HBM, VM, VM, VM, VM, SM, VM, HBM, HBM],
        out_specs=(VM, VM),
        scratch_shapes=[
            vm(4, 64, 2048), vm(256, 2048),
            vm(2048, 512), vm(2048, 512), vm(2048, 512), vm(2048, 128), vm(2048, 128),
            vm(512, 2048), vm(512, 2048),
            vm(256, 512), vm(2, 128, 256), vm(256, 256), vm(256, 256),
            vm(2, 2, NX, NZ, 128, 256), vm(256, 256), vm(2, 4, 256, 128),
            vm(2, 4, 256, 128, dtype=F32), vm(2, 4, 256, 128, dtype=F32), vm(2, 4, 256, 128, dtype=F32),
            vm(32, 512), vm(4, 288, 128, dtype=F32), vm(4, 256, 128, dtype=F32),
            vm(256, 128, dtype=F32), vm(3, 256, 128, dtype=F32),
            vm(256, 256), vm(256, 512), vm(256, 256), vm(256, 256),
            vm(8, 256, dtype=F32), vm(8, 256, dtype=F32), vm(8, 256, dtype=F32),
            vm(256, 2048, dtype=F32), vm(2, 64, 1024), vm(2, 64, 1024), vm(2, 64, 1024), vm(2, 64, 1024),
            vm(2, 2, 64, 1024),
            dma((7,)), dma, dma((2, 2)), dma((2, 2)), dma((2,)), dma((2,)),
            dma((2,)),
            dma((2, 2)), dma((2, 2)),
            dma((4, 2, 2)), dma((4, 2, 2)),
            dma((4, 2, 2)), dma((4, 2, 2)),
            dma((2, 5, 2, 2)), dma((2, 5, 2, 2)),
            dma((2, 5, 2)), dma((2, 5, 2)),
            dma((4,)), dma((4,)),
            dma((3,)), dma((3,)),
            dma((2,)), dma((2,)), dma((2, 2)), dma((2, 2)),
        ],
        compiler_params=pltpu.CompilerParams(
            collective_id=0, has_side_effects=True, vmem_limit_bytes=60 * 1024 * 1024
        ),
        name="layer",
    )(
        tokens, norm_gain.reshape(1, -1), w_glu_a, w_glu_b, w_query, w_key, w_value, query_gain, key_gain,
        conv_taps, ln_gain.reshape(1, -1), lam_head, sub_gain.reshape(1, -1), w_out_conv, w_out_attn,
    )


def solution(mesh):
    return jax.shard_map(
        on_device,
        mesh=mesh,
        in_specs=(
            P(("sp", "tp"), None), P(), P(None, "tp"), P(None, "tp"), P(None, "tp"), P("tp"),
            P(None, "tp"), P(None, "tp"), P(None, "tp"), P("tp", None), P("tp", None), P("tp"),
            P(), P("tp", None), P("tp", None),
        ),
        out_specs=(P(("sp", "tp"), None), P(None, "tp", "sp")),
        check_vma=False,
    )
```

```python
import functools

import jax
import jax.numpy as jnp
from jax import lax
from jax.experimental import pallas as pl
from jax.experimental.pallas import tpu as pltpu
from jax.sharding import PartitionSpec as P

KW = 31
MESH = pl.DeviceIdType.MESH
NZ, NX, NT = 8, 4, 4
BF, F32 = jnp.bfloat16, jnp.float32
VM = pl.BlockSpec(memory_space=pltpu.VMEM)


def remote(src, dst, send, recv, device):
    return pltpu.make_async_remote_copy(
        src_ref=src, dst_ref=dst, send_sem=send, recv_sem=recv, device_id=device, device_id_type=MESH
    )


def greet(devices):
    barrier = pltpu.get_barrier_semaphore()
    for device in devices:
        pl.semaphore_signal(barrier, inc=1, device_id=device, device_id_type=MESH)
    return lambda: pl.semaphore_wait(barrier, len(devices))


def half_norm(value, gain):
    low = lax.broadcasted_iota(jnp.int32, value.shape, 1) < 64
    squares = value * value
    first = jnp.sum(jnp.where(low, squares, 0.0), axis=1, keepdims=True)
    second = jnp.sum(jnp.where(low, 0.0, squares), axis=1, keepdims=True)
    scale = jnp.where(low, lax.rsqrt(first / 64 + 1e-6), lax.rsqrt(second / 64 + 1e-6))
    return (value * scale * gain).astype(BF)


HBM = pl.BlockSpec(memory_space=pltpu.MemorySpace.HBM)
SM = pl.BlockSpec(memory_space=pltpu.SMEM)


def layer_kernel(
    tok, gain, wa_h, wb_h, wq_h, wk_h, wv_h, qg, kg, taps, ln_gain, lam, sub_gain, wc_h, wo_h,
    mixed, logs,
    rows, normed, wa, wb, wq, wk, wv, wc, wo, gated, q_own, q_far,
    kv, q_in, qpad, m_ref, l_ref, acc, halo, gpad, csum, stat_out, stat_in,
    attn, conv_out, ret_out, ret_in, log_out, log_in, log_self,
    part, far, near, total_out, r1, r2,
    w_sem, own_sem, y1s, y1r, y2s, y2r,
    ax_s, ax_r, az_s, az_r, bz_s, bz_r, bx_s, bx_r, dd_s, dd_r, ex_s, ex_r, st_s, st_r,
    o1s, o1r, o2s, o2r,
):
    sp, y = lax.axis_index("sp"), lax.axis_index("tp")
    z, x, c = sp // 8, lax.rem(sp // 2, 4), lax.rem(sp, 2)
    sib = 1 - c

    def zm(value):
        return lax.rem(value + 2 * NZ, NZ)

    def xm(value):
        return lax.rem(value + 2 * NX, NX)

    def at(zz, xx, cc):
        return {"sp": zz * 8 + xx * 2 + cc, "tp": y}

    zdev = (at(zm(z + 1), x, c), at(zm(z - 1), x, c))
    xdev = (at(z, xm(x + 1), c), at(z, xm(x - 1), c))
    sdev = at(z, x, sib)
    far_z = NZ - 1 - z
    pdev = at(far_z, x, c)
    nxt = {"sp": lax.rem(sp + 1, 64), "tp": y}
    prv = {"sp": lax.rem(sp + 63, 64), "tp": y}
    ydev = [{"sp": sp, "tp": lax.rem(y + k, NT)} for k in (1, 2, 3)]
    up, down = ydev[0], ydev[2]
    meet = greet([*zdev, *xdev, sdev, pdev, nxt, prv, *ydev])
    sends = []

    def go(copy):
        copy.start()
        sends.append(copy)

    def origin(s, d):
        return zm(z - s) if d == 0 else zm(z + s)

    def signs(s):
        return (0, 1) if 0 < s < 4 else (0,)

    def ways(s, i):
        return (0, 1) if s < 4 else (i,)

    offsets = (0, -1, 1, 2)

    def ax1(a, d, landing):
        ref = kv.at[c, a, xm(x - 1 + 2 * d) if landing else x, z]
        return remote(ref, ref, ax_s.at[0, a, d], ax_r.at[0, a, d], xdev[d])

    def ax2(a, landing):
        ref = kv.at[c, a, xm(x + 2) if landing else xm(x - 1 + 2 * a), z]
        return remote(ref, ref, ax_s.at[1, a, 0], ax_r.at[1, a, 0], xdev[a])

    def az(a, s, d, j, landing):
        ref = kv.at[c, a, xm(x + offsets[j]), origin(s if landing else s - 1, d)]
        return remote(ref, ref, az_s.at[a, s - 1, d, j], az_r.at[a, s - 1, d, j], zdev[d])

    def bz(i, s, d, landing):
        ref = kv.at[c, 2 + i, x, origin(s if landing else s - 1, d)]
        return remote(ref, ref, bz_s.at[i, s - 1, d], bz_r.at[i, s - 1, d], zdev[d])

    def bx1(i, s, g, d, landing):
        ref = kv.at[c, 2 + i, xm(x - 1 + 2 * d) if landing else x, origin(s, g)]
        return remote(ref, ref, bx_s.at[i, s, g, d], bx_r.at[i, s, g, d], xdev[d])

    def bx2(i, s, g, landing):
        ref = kv.at[c, 2 + i, xm(x + 2) if landing else xm(x - 1 + 2 * i), origin(s, g)]
        return remote(ref, ref, bx_s.at[i, s, g, 2], bx_r.at[i, s, g, 2], xdev[i])

    def dd(h, s, g, landing):
        ref = kv.at[sib if landing else c, pl.ds(2 * h, 2), :, origin(s, g)]
        return remote(ref, ref, dd_s.at[h, s, g], dd_r.at[h, s, g], sdev)

    def a_begin(a):
        for d in range(2):
            go(ax1(a, d, False))
        for d in range(2):
            go(az(a, 1, d, 0, False))

    def a_x1(a):
        for d in range(2):
            ax1(a, d, True).wait_recv()
        go(ax2(a, False))
        for j in (1, 2):
            for d in range(2):
                go(az(a, 1, d, j, False))

    def a_x2(a):
        ax2(a, True).wait_recv()
        for d in range(2):
            go(az(a, 1, d, 3, False))

    def a_z(a, s):
        for j in range(4):
            for d in ways(s, a):
                az(a, s, d, j, True).wait_recv()
                if s < 3 or (s == 3 and d == a):
                    go(az(a, s + 1, d, j, False))

    def b_begin(i):
        for d in range(2):
            go(bz(i, 1, d, False))
        for d in range(2):
            go(bx1(i, 0, 0, d, False))

    def b_z(i, s):
        for d in ways(s, i):
            bz(i, s, d, True).wait_recv()
            if s < 3 or (s == 3 and d == i):
                go(bz(i, s + 1, d, False))
            for way in range(2):
                go(bx1(i, s, d if s < 4 else 0, way, False))

    def b_x1(i, s):
        for g in signs(s):
            for d in range(2):
                bx1(i, s, g, d, True).wait_recv()
            go(bx2(i, s, g, False))

    def b_x2(i, s):
        for g in signs(s):
            bx2(i, s, g, True).wait_recv()

    def dd_send(h, s):
        for g in signs(s):
            go(dd(h, s, g, False))

    def dd_recv(s):
        for h in range(2):
            for g in signs(s):
                dd(h, s, g, True).wait_recv()

    slot_rows = [lax.rem(y + k, NT) for k in (0, 3, 1, 2)]

    def tile(which, cc, zt, masked):
        pieces = [(j, k) for j in range(4) for k in range(NX)]
        keys = jnp.concatenate([kv[cc, j, k, zt, :, 0:128] for j, k in pieces], axis=0)
        values = jnp.concatenate([kv[cc, j, k, zt, :, 128:256] for j, k in pieces], axis=0)
        if masked:
            row = lax.broadcasted_iota(jnp.int32, (256, 128), 0) + (x * 512 + c * 256)
            col = lax.broadcasted_iota(jnp.int32, (256, 128), 1)
            col = jnp.where(col < 64, col, col + 448) + cc * 256
        scores = [
            lax.dot_general(
                qpad[which, pl.ds(2 * n, 2)].reshape(512, 128),
                keys,
                (((1,), (1,)), ((), ())),
                preferred_element_type=F32,
            )
            for n in range(2)
        ]
        for n in range(2):
            weights, fades = [], []
            for k in range(2):
                hm = 2 * n + k
                parts = [scores[n][k * 256 : (k + 1) * 256, p * 128 : (p + 1) * 128] for p in range(8)]
                if masked:
                    parts = [
                        jnp.where(col + ((p % 2) * 1024 + slot_rows[p // 2] * 64) <= row, item, -1e30)
                        for p, item in enumerate(parts)
                    ]
                old = m_ref[which, hm]
                new = jnp.maximum(old, jnp.max(functools.reduce(jnp.maximum, parts), axis=1, keepdims=True))
                fade = jnp.exp(old - new)
                parts = [jnp.exp(item - new) for item in parts]
                m_ref[which, hm] = new
                l_ref[which, hm] = l_ref[which, hm] * fade + functools.reduce(jnp.add, parts)
                weights.append(jnp.concatenate([item.astype(BF) for item in parts], axis=1))
                fades.append(fade)
            outs = jnp.dot(jnp.concatenate(weights, axis=0), values, preferred_element_type=F32)
            for k in range(2):
                hm = 2 * n + k
                acc[which, hm] = acc[which, hm] * fades[k] + outs[k * 256 : (k + 1) * 256]

    early = z < NZ // 2

    def attend(s, g):
        zt = zm(z - s + 2 * s * g)

        def step(i, carry):
            which = lax.rem(i, 2)
            cc = lax.rem(c + i // 2, 2)
            zq = jnp.where(which == 0, z, far_z)

            @pl.when(zt < zq)
            def _():
                tile(which, cc, zt, False)

            if s in (1, 3):

                @pl.when(zt == zq)
                def _():
                    tile(which, cc, zt, True)

            return carry

        lax.fori_loop(0, 4, step, 0)

    def attend_first(cc):
        @pl.when(early)
        def _():
            tile(1, cc, z, False)

        @pl.when(jnp.logical_not(early))
        def _():
            tile(0, cc, z, True)

    def attend_last():
        def step(cc, carry):
            @pl.when(early)
            def _():
                tile(0, cc, z, True)

            return carry

        lax.fori_loop(0, 2, step, 0)

    def events_a(t):
        if t + 1 <= 4:
            for i in range(2):
                b_z(i, t + 1)
        for i in range(2):
            b_x1(i, t)
        a_z(0, t)

    def events_b(t):
        a_z(1, t)
        dd_send(0, t)
        for i in range(2):
            b_x2(i, t)
        dd_send(1, t)

    pairs = ((wk_h, wk), (wv_h, wv), (wq_h, wq), (wa_h, wa), (wb_h, wb), (wc_h, wc), (wo_h, wo))
    loads = [pltpu.make_async_copy(src, dst, w_sem.at[i]) for i, (src, dst) in enumerate(pairs)]
    own_rows = pltpu.make_async_copy(tok, rows.at[y], own_sem)
    own_rows.start()
    meet()

    def piece(slot, half):
        return rows.at[slot, pl.ds(half * 32, 32)]

    ypair = ((up, lax.rem(y + 3, NT)), (down, lax.rem(y + 1, NT)))
    for order in range(2):
        for d in range(2):
            half = order if d == 0 else 1 - order
            go(remote(tok.at[pl.ds(half * 32, 32)], piece(y, half), y1s.at[d, half], y1r.at[d, half], ypair[d][0]))
    for load in loads:
        load.start()
    own_rows.wait()

    def norm_slot(slot):
        value = rows[slot].astype(F32)
        scale = lax.rsqrt(jnp.mean(value * value, axis=1, keepdims=True) + 1e-6)
        normed[pl.ds(pl.multiple_of(slot * 64, 64), 64), :] = (value * scale * gain[...]).astype(BF)

    def dot(weight):
        return jnp.dot(normed[...], weight, preferred_element_type=F32)

    def key_slot(j, slot):
        at_rows = pl.ds(pl.multiple_of(slot * 64, 64), 64)
        norm_slot(slot)
        value = normed[at_rows, :]
        keys = jnp.dot(value, wk[...], preferred_element_type=F32)
        kv[c, j, x, z, :, 128:256] = jnp.dot(value, wv[...], preferred_element_type=F32).astype(BF)
        kv[c, j, x, z, :, 0:128] = half_norm(keys, kg[...])

    for load in loads[:2]:
        load.wait()
    key_slot(0, y)
    m_ref[...] = jnp.full(m_ref.shape, -1e30, F32)
    a_begin(0)
    l_ref[...] = jnp.zeros(l_ref.shape, F32)
    acc[...] = jnp.zeros(acc.shape, F32)
    for d in range(2):
        target, source = ypair[d]
        ref = piece(source, d)
        remote(ref, ref, y1s.at[d, d], y1r.at[d, d], target).wait_recv()
        go(remote(ref, ref, y2s.at[d], y2r.at[d], target))
    for d in range(2):
        target, source = ypair[d]
        ref = piece(source, 1 - d)
        remote(ref, ref, y1s.at[d, 1 - d], y1r.at[d, 1 - d], target).wait_recv()
        key_slot(1 + d, source)
        if d == 0:
            a_begin(1)
            a_x1(0)
        else:
            b_begin(0)
    a_x2(0)
    opposite = lax.rem(y + 2, NT)
    for d in range(2):
        ref = piece(opposite, d)
        remote(ref, ref, y2s.at[d], y2r.at[d], ypair[d][0]).wait_recv()
    key_slot(3, opposite)
    b_begin(1)
    a_x1(1)

    def project_q(n, target):
        queries = dot(wq[:, n * 256 : (n + 1) * 256])
        for k in range(2):
            one = half_norm(queries[:, k * 128 : (k + 1) * 128], qg[2 * n + k : 2 * n + k + 1, :])
            target[:, k * 128 : (k + 1) * 128] = one * jnp.asarray(0.125, BF)

    for load in loads[2:5]:
        load.wait()
    project_q(1, q_far)
    b_z(0, 1)
    b_x1(0, 0)
    a_x2(1)
    dd_send(0, 0)
    for n in range(2):
        span = slice(n * 256, (n + 1) * 256)
        gated[:, span] = (dot(wa[:, span]) * jax.nn.sigmoid(dot(wb[:, span]))).astype(BF)
    q_copy = remote(q_far, q_in, ex_s.at[0], ex_r.at[0], pdev)
    go(q_copy)
    b_x1(1, 0)
    b_x2(0, 0)
    b_z(1, 1)
    project_q(0, q_own)
    halo_copy = remote(gated.at[pl.ds(224, 32)], halo, ex_s.at[1], ex_r.at[1], nxt)
    go(halo_copy)
    b_x2(1, 0)
    dd_send(1, 0)
    low = lax.broadcasted_iota(jnp.int32, (256, 128), 1) < 64

    def pad(which, source):
        for k in range(2):
            head = source[:, k * 128 : (k + 1) * 128].astype(F32)
            qpad[which, 2 * k] = jnp.where(low, head, 0.0).astype(BF)
            qpad[which, 2 * k + 1] = jnp.where(low, 0.0, head).astype(BF)

    pad(0, q_own)
    for k in range(4):
        gpad[k, 32:288, :] = gated[:, k * 128 : (k + 1) * 128].astype(F32)
    halo_copy.wait_recv()
    for k in range(4):
        gpad[k, 0:32, :] = jnp.where(sp > 0, halo[:, k * 128 : (k + 1) * 128].astype(F32), 0.0)

    def conv_step(k, carry):
        one, two = carry
        total = jnp.zeros((256, 128), F32)
        lanes = pl.ds(pl.multiple_of(k * 128, 128), 128)
        for j in range(KW):
            total = total + taps[j : j + 1, lanes] * gpad[k, j + 2 : j + 258, :]
        csum[k] = total
        return one + total, two + total * total

    nothing = jnp.zeros((256, 128), F32)
    one, two = lax.fori_loop(0, 4, conv_step, (nothing, nothing))
    lane = lax.broadcasted_iota(jnp.int32, (256, 128), 1)
    stat_out[...] = jnp.where(
        lane == 0, jnp.sum(one, axis=1, keepdims=True), jnp.sum(two, axis=1, keepdims=True)
    )
    q_copy.wait_recv()
    pad(1, q_in)
    for k in range(3):
        go(remote(stat_out, stat_in.at[k], st_s.at[k], st_r.at[k], ydev[k]))
    attend_first(c)
    events_a(1)
    dd_recv(0)
    attend_first(sib)
    events_b(1)
    for k in range(3):
        remote(stat_out, stat_in.at[k], st_s.at[k], st_r.at[k], ydev[k]).wait_recv()
    total = (stat_out[...] + stat_in[0]) + (stat_in[1] + stat_in[2])
    mean = total[:, 0:1] / (NT * 512)
    mean_sq = total[:, 1:2] / (NT * 512)
    scale = lax.rsqrt(mean_sq - mean * mean + 1e-5)
    for k in range(4):
        span = slice(k * 128, (k + 1) * 128)
        conv_out[:, span] = jax.nn.silu((csum[k] - mean) * scale * ln_gain[:, span]).astype(BF)
    for load in loads[5:]:
        load.wait()
    for n in range(4):
        span = pl.ds(n * 512, 512)
        part[:, span] = jnp.dot(conv_out[...], wc[:, span], preferred_element_type=F32)

    for t in range(1, 5):
        if t < 4:
            events_a(t + 1)
        dd_recv(t)
        attend(t, 0)
        if t < 4:
            events_b(t + 1)
            attend(t, 1)

    def finish(which, out_ref, log_ref):
        table = jnp.zeros((256, 128), F32)
        for k in range(2):
            outs = []
            for m in range(2):
                total = jnp.sum(l_ref[which, 2 * k + m], axis=1, keepdims=True)
                outs.append(acc[which, 2 * k + m] / total)
                table = jnp.where(lane == 2 * k + m, m_ref[which, 2 * k + m] + jnp.log(total), table)
            row = 2 * which + k
            diff = outs[0] - lam[row] * outs[1]
            scale = lax.rsqrt(jnp.mean(diff * diff, axis=1, keepdims=True) + 1e-6)
            out_ref[:, k * 128 : (k + 1) * 128] = (diff * scale * sub_gain[...]).astype(BF)
        log_ref[...] = table.T[0:8, :]

    finish(1, ret_out, log_out)
    back = [
        remote(ret_out, ret_in, ex_s.at[2], ex_r.at[2], pdev),
        remote(log_out, log_in, ex_s.at[3], ex_r.at[3], pdev),
    ]
    for copy in back:
        go(copy)
    attend_last()
    finish(0, attn, log_self)
    for n in range(4):
        span = pl.ds(n * 512, 512)
        part[:, span] += jnp.dot(attn[...], wo[0:256, span], preferred_element_type=F32)
    for copy in back:
        copy.wait_recv()
    for which, table in ((0, log_self), (1, log_in)):
        for k in range(2):
            for m in range(2):
                logs[m, 2 * which + k : 2 * which + k + 1, :] = table[2 * k + m : 2 * k + m + 1, :]

    targets = (up, down)
    blocks = (lax.rem(y + 1, NT), lax.rem(y + 3, NT))

    def block_rows(block):
        return pl.ds(pl.multiple_of(block * 64, 64), 64)

    for n in range(4):
        span = pl.ds(n * 512, 512)
        part[:, span] += jnp.dot(ret_in[...], wo[256:512, span], preferred_element_type=F32)
        if n % 2 == 1:
            d = n // 2
            wide = pl.ds(d * 1024, 1024)
            far[d] = part[block_rows(opposite), wide].astype(BF)
            near[d] = part[block_rows(blocks[1 - d]), wide].astype(BF)
            go(remote(far.at[d], r1.at[d], o1s.at[d], o1r.at[d], targets[d]))
            go(remote(near.at[d], r2.at[1 - d, d], o2s.at[1 - d, d], o2r.at[1 - d, d], targets[1 - d]))
    for d in range(2):
        remote(far.at[d], r1.at[d], o1s.at[d], o1r.at[d], targets[d]).wait_recv()
        wide = pl.ds(d * 1024, 1024)
        total_out[d] = (part[block_rows(blocks[d]), wide] + r1[d].astype(F32)).astype(BF)
        go(remote(total_out.at[d], r2.at[d, d], o2s.at[d, d], o2r.at[d, d], targets[d]))
    for d in (1, 0):
        for k in (1 - d, d):
            remote(total_out.at[d], r2.at[k, d], o2s.at[k, d], o2r.at[k, d], targets[k]).wait_recv()
        wide = pl.ds(d * 1024, 1024)
        mixed[:, wide] = (part[block_rows(y), wide] + (r2[0, d].astype(F32) + r2[1, d].astype(F32))).astype(BF)
    for copy in sends:
        copy.wait_send()


def on_device(
    tokens, norm_gain, w_glu_a, w_glu_b, conv_taps, ln_gain, w_query, w_key, w_value,
    query_gain, key_gain, lam_head, sub_gain, w_out_conv, w_out_attn,
):
    dma = pltpu.SemaphoreType.DMA

    def vm(*shape, dtype=BF):
        return pltpu.VMEM(shape, dtype)

    return pl.pallas_call(
        layer_kernel,
        out_shape=(jax.ShapeDtypeStruct((64, 2048), BF), jax.ShapeDtypeStruct((2, 4, 256), F32)),
        in_specs=[VM, VM, HBM, HBM, HBM, HBM, HBM, VM, VM, VM, VM, SM, VM, HBM, HBM],
        out_specs=(VM, VM),
        scratch_shapes=[
            vm(4, 64, 2048), vm(256, 2048),
            vm(2048, 512), vm(2048, 512), vm(2048, 512), vm(2048, 128), vm(2048, 128),
            vm(512, 2048), vm(512, 2048),
            vm(256, 512), vm(256, 256), vm(256, 256),
            vm(2, 4, NX, NZ, 64, 256), vm(256, 256), vm(2, 4, 256, 128),
            vm(2, 4, 256, 128, dtype=F32), vm(2, 4, 256, 128, dtype=F32), vm(2, 4, 256, 128, dtype=F32),
            vm(32, 512), vm(4, 288, 128, dtype=F32), vm(4, 256, 128, dtype=F32),
            vm(256, 128, dtype=F32), vm(3, 256, 128, dtype=F32),
            vm(256, 256), vm(256, 512), vm(256, 256), vm(256, 256),
            vm(8, 256, dtype=F32), vm(8, 256, dtype=F32), vm(8, 256, dtype=F32),
            vm(256, 2048, dtype=F32), vm(2, 64, 1024), vm(2, 64, 1024), vm(2, 64, 1024), vm(2, 64, 1024),
            vm(2, 2, 64, 1024),
            dma((7,)), dma, dma((2, 2)), dma((2, 2)), dma((2,)), dma((2,)),
            dma((2, 2, 2)), dma((2, 2, 2)),
            dma((2, 4, 2, 4)), dma((2, 4, 2, 4)),
            dma((2, 4, 2)), dma((2, 4, 2)),
            dma((2, 5, 2, 3)), dma((2, 5, 2, 3)),
            dma((2, 5, 2)), dma((2, 5, 2)),
            dma((4,)), dma((4,)),
            dma((3,)), dma((3,)),
            dma((2,)), dma((2,)), dma((2, 2)), dma((2, 2)),
        ],
        compiler_params=pltpu.CompilerParams(
            collective_id=0, has_side_effects=True, vmem_limit_bytes=60 * 1024 * 1024
        ),
        name="layer",
    )(
        tokens, norm_gain.reshape(1, -1), w_glu_a, w_glu_b, w_query, w_key, w_value, query_gain, key_gain,
        conv_taps, ln_gain.reshape(1, -1), lam_head, sub_gain.reshape(1, -1), w_out_conv, w_out_attn,
    )


def solution(mesh):
    return jax.shard_map(
        on_device,
        mesh=mesh,
        in_specs=(
            P(("sp", "tp"), None), P(), P(None, "tp"), P(None, "tp"), P(None, "tp"), P("tp"),
            P(None, "tp"), P(None, "tp"), P(None, "tp"), P("tp", None), P("tp", None), P("tp"),
            P(), P("tp", None), P("tp", None),
        ),
        out_specs=(P(("sp", "tp"), None), P(None, "tp", "sp")),
        check_vma=False,
    )
```

```python
import functools

import jax
import jax.numpy as jnp
from jax import lax
from jax.experimental import pallas as pl
from jax.experimental.pallas import tpu as pltpu
from jax.sharding import PartitionSpec as P

KW = 31
MESH = pl.DeviceIdType.MESH
NZ, NX, NT = 8, 4, 4
BF, F32 = jnp.bfloat16, jnp.float32
VM = pl.BlockSpec(memory_space=pltpu.VMEM)


def remote(src, dst, send, recv, device):
    return pltpu.make_async_remote_copy(
        src_ref=src, dst_ref=dst, send_sem=send, recv_sem=recv, device_id=device, device_id_type=MESH
    )


def greet(devices):
    barrier = pltpu.get_barrier_semaphore()
    for device in devices:
        pl.semaphore_signal(barrier, inc=1, device_id=device, device_id_type=MESH)
    return lambda: pl.semaphore_wait(barrier, len(devices))


def half_norm(value, gain):
    low = lax.broadcasted_iota(jnp.int32, value.shape, 1) < 64
    squares = value * value
    first = jnp.sum(jnp.where(low, squares, 0.0), axis=1, keepdims=True)
    second = jnp.sum(jnp.where(low, 0.0, squares), axis=1, keepdims=True)
    scale = jnp.where(low, lax.rsqrt(first / 64 + 1e-6), lax.rsqrt(second / 64 + 1e-6))
    return (value * scale * gain).astype(BF)


HBM = pl.BlockSpec(memory_space=pltpu.MemorySpace.HBM)
SM = pl.BlockSpec(memory_space=pltpu.SMEM)


def layer_kernel(
    tok, gain, wa_h, wb_h, wq_h, wk_h, wv_h, qg, kg, taps, ln_gain, lam, sub_gain, wc_h, wo_h,
    mixed, logs,
    rows, normed, wa, wb, wq, wk, wv, wc, wo, gated, q_own, q_far,
    kv, q_in, qpad, m_ref, l_ref, acc, halo, gpad, csum, stat_out, stat_in,
    attn, conv_out, ret_out, ret_in, log_out, log_in, log_self,
    part, far, near, total_out, r1, r2,
    w_sem, own_sem, y1s, y1r, y2s, y2r,
    ax_s, ax_r, az_s, az_r, bz_s, bz_r, bx_s, bx_r, dd_s, dd_r, ex_s, ex_r, st_s, st_r,
    o1s, o1r, o2s, o2r,
):
    sp, y = lax.axis_index("sp"), lax.axis_index("tp")
    z, x, c = sp // 8, lax.rem(sp // 2, 4), lax.rem(sp, 2)
    sib = 1 - c

    def zm(value):
        return lax.rem(value + 2 * NZ, NZ)

    def xm(value):
        return lax.rem(value + 2 * NX, NX)

    def at(zz, xx, cc):
        return {"sp": zz * 8 + xx * 2 + cc, "tp": y}

    zdev = (at(zm(z + 1), x, c), at(zm(z - 1), x, c))
    xdev = (at(z, xm(x + 1), c), at(z, xm(x - 1), c))
    sdev = at(z, x, sib)
    far_z = NZ - 1 - z
    pdev = at(far_z, x, c)
    nxt = {"sp": lax.rem(sp + 1, 64), "tp": y}
    prv = {"sp": lax.rem(sp + 63, 64), "tp": y}
    ydev = [{"sp": sp, "tp": lax.rem(y + k, NT)} for k in (1, 2, 3)]
    up, down = ydev[0], ydev[2]
    meet = greet([*zdev, *xdev, sdev, pdev, nxt, prv, *ydev])
    sends = []

    def go(copy, keep=True):
        copy.start()
        if keep:
            sends.append(copy)

    def origin(s, d):
        return zm(z - s) if d == 0 else zm(z + s)

    def signs(s):
        return (0, 1) if 0 < s < 4 else (0,)

    def ways(s, i):
        return (0, 1) if s < 4 else (i,)

    offsets = (0, -1, 1, 2)

    def ax1(a, d):
        ref = kv.at[c, a, x, z]
        go(remote(ref, ref, ax_s, ax_r.at[a, 0], xdev[d]), False)

    def ax2(a):
        ref = kv.at[c, a, xm(x - 1 + 2 * a), z]
        go(remote(ref, ref, ax_s, ax_r.at[a, 1], xdev[a]), False)

    def az(a, s, d, j):
        ref = kv.at[c, a, xm(x + offsets[j]) if s == 1 else slice(None), origin(s - 1, d)]
        go(remote(ref, ref, az_s, az_r.at[a, s - 1, d], zdev[d]), False)

    def bz(i, s, d, landing):
        ref = kv.at[c, 2 + i, x, origin(s if landing else s - 1, d)]
        return remote(ref, ref, bz_s, bz_r.at[i, s - 1, d], zdev[d])

    def bx1(i, s, g, d):
        ref = kv.at[c, 2 + i, x, origin(s, g)]
        go(remote(ref, ref, bx_s, bx_r.at[i, s, g, 0], xdev[d]), False)

    def bx2(i, s, g, landing):
        ref = kv.at[c, 2 + i, xm(x + 2) if landing else xm(x - 1 + 2 * i), origin(s, g)]
        return remote(ref, ref, bx_s, bx_r.at[i, s, g, 1], xdev[i])

    def taken(ref, send, recv):
        remote(ref, ref, send, recv, sdev).wait_recv()

    def a_begin(a):
        for d in range(2):
            ax1(a, d)
        for d in range(2):
            az(a, 1, d, 0)

    def a_x1(a):
        taken(kv.at[c, a, pl.ds(0, 2), z], ax_s, ax_r.at[a, 0])
        ax2(a)
        for j in (1, 2):
            for d in range(2):
                az(a, 1, d, j)

    def a_x2(a):
        taken(kv.at[c, a, 0, z], ax_s, ax_r.at[a, 1])
        for d in range(2):
            az(a, 1, d, 3)

    def a_z(a, s):
        for d in ways(s, a):
            taken(kv.at[c, a, :, origin(s, d)], az_s, az_r.at[a, s - 1, d])
            if s < 3 or (s == 3 and d == a):
                az(a, s + 1, d, 0)

    def b_begin(i):
        for d in range(2):
            go(bz(i, 1, d, False), False)
        for d in range(2):
            bx1(i, 0, 0, d)

    def b_z(i, s):
        for d in ways(s, i):
            bz(i, s, d, True).wait_recv()
            if s < 3 or (s == 3 and d == i):
                go(bz(i, s + 1, d, False), False)
            for way in range(2):
                bx1(i, s, d if s < 4 else 0, way)

    def b_x1(i, s):
        for g in signs(s):
            taken(kv.at[c, 2 + i, pl.ds(0, 2), origin(s, g)], bx_s, bx_r.at[i, s, g, 0])
            go(bx2(i, s, g, False), False)

    def b_x2(i, s):
        for g in signs(s):
            bx2(i, s, g, True).wait_recv()

    def dd_send(h, s):
        for g in signs(s):
            ref = kv.at[c, pl.ds(2 * h, 2), :, origin(s, g)]
            go(remote(ref, ref, dd_s, dd_r.at[s, g], sdev), False)

    def dd_recv(s):
        for g in signs(s):
            taken(kv.at[sib, :, :, origin(s, g)], dd_s, dd_r.at[s, g])

    def all_sent():
        for ref, sem in (
            (kv.at[c, pl.ds(0, 3), pl.ds(0, 2), 0], ax_s),
            (kv.at[c, pl.ds(0, 2), :, pl.ds(0, 7)], az_s),
            (kv.at[c, pl.ds(0, 2), 0, pl.ds(0, 7)], bz_s),
            (kv.at[c, :, :, pl.ds(0, 3)], bx_s),
            (kv.at[c], dd_s),
        ):
            remote(ref, ref, sem, ax_r.at[0, 0], sdev).wait_send()

    slot_rows = [lax.rem(y + k, NT) for k in (0, 3, 1, 2)]

    def tile(which, cc, zt, masked):
        pieces = [(j, k) for j in range(4) for k in range(NX)]
        keys = jnp.concatenate([kv[cc, j, k, zt, :, 0:128] for j, k in pieces], axis=0)
        values = jnp.concatenate([kv[cc, j, k, zt, :, 128:256] for j, k in pieces], axis=0)
        if masked:
            row = lax.broadcasted_iota(jnp.int32, (256, 128), 0) + (x * 512 + c * 256)
            col = lax.broadcasted_iota(jnp.int32, (256, 128), 1)
            col = jnp.where(col < 64, col, col + 448) + cc * 256
        scores = [
            lax.dot_general(
                qpad[which, pl.ds(2 * n, 2)].reshape(512, 128),
                keys,
                (((1,), (1,)), ((), ())),
                preferred_element_type=F32,
            )
            for n in range(2)
        ]
        for n in range(2):
            weights, fades = [], []
            for k in range(2):
                hm = 2 * n + k
                parts = [scores[n][k * 256 : (k + 1) * 256, p * 128 : (p + 1) * 128] for p in range(8)]
                if masked:
                    parts = [
                        jnp.where(col + ((p % 2) * 1024 + slot_rows[p // 2] * 64) <= row, item, -1e30)
                        for p, item in enumerate(parts)
                    ]
                old = m_ref[which, hm]
                new = jnp.maximum(old, jnp.max(functools.reduce(jnp.maximum, parts), axis=1, keepdims=True))
                fade = jnp.exp(old - new)
                parts = [jnp.exp(item - new) for item in parts]
                m_ref[which, hm] = new
                l_ref[which, hm] = l_ref[which, hm] * fade + functools.reduce(jnp.add, parts)
                weights.append(jnp.concatenate([item.astype(BF) for item in parts], axis=1))
                fades.append(fade)
            outs = jnp.dot(jnp.concatenate(weights, axis=0), values, preferred_element_type=F32)
            for k in range(2):
                hm = 2 * n + k
                acc[which, hm] = acc[which, hm] * fades[k] + outs[k * 256 : (k + 1) * 256]

    early = z < NZ // 2

    def attend(s, g, first=0, last=4):
        zt = zm(z - s + 2 * s * g)

        def step(i, carry):
            which = 1 - i // 2
            cc = lax.rem(c + i, 2)
            zq = jnp.where(which == 0, z, far_z)

            @pl.when(zt < zq)
            def _():
                tile(which, cc, zt, False)

            if s in (1, 3):

                @pl.when(zt == zq)
                def _():
                    tile(which, cc, zt, True)

            return carry

        lax.fori_loop(first, last, step, 0)

    def attend_first(cc):
        @pl.when(early)
        def _():
            tile(1, cc, z, False)

        @pl.when(jnp.logical_not(early))
        def _():
            tile(0, cc, z, True)

    def attend_last():
        def step(cc, carry):
            @pl.when(early)
            def _():
                tile(0, cc, z, True)

            return carry

        lax.fori_loop(0, 2, step, 0)

    def events_a(t):
        if t + 1 <= 4:
            for i in range(2):
                b_z(i, t + 1)
        a_z(0, t)

    def events_b(t):
        a_z(1, t)
        dd_send(0, t)
        if t + 1 <= 4:
            for i in range(2):
                b_x1(i, t + 1)
        for i in range(2):
            b_x2(i, t)
        dd_send(1, t)

    pairs = ((wk_h, wk), (wv_h, wv), (wq_h, wq), (wa_h, wa), (wb_h, wb), (wc_h, wc), (wo_h, wo))
    loads = [pltpu.make_async_copy(src, dst, w_sem.at[i]) for i, (src, dst) in enumerate(pairs)]
    own_rows = pltpu.make_async_copy(tok, rows.at[y], own_sem)
    own_rows.start()
    for load in loads[:2]:
        load.start()
    meet()

    def piece(slot, half):
        return rows.at[slot, pl.ds(half * 32, 32)]

    ypair = ((up, lax.rem(y + 3, NT)), (down, lax.rem(y + 1, NT)))
    for order in range(2):
        for d in range(2):
            half = order if d == 0 else 1 - order
            go(remote(tok.at[pl.ds(half * 32, 32)], piece(y, half), y1s.at[d, half], y1r.at[d, half], ypair[d][0]))
    for load in loads[2:]:
        load.start()
    own_rows.wait()

    def norm_slot(slot):
        value = rows[slot].astype(F32)
        scale = lax.rsqrt(jnp.mean(value * value, axis=1, keepdims=True) + 1e-6)
        normed[pl.ds(pl.multiple_of(slot * 64, 64), 64), :] = (value * scale * gain[...]).astype(BF)

    def dot(weight):
        return jnp.dot(normed[...], weight, preferred_element_type=F32)

    def key_slot(j, slot):
        at_rows = pl.ds(pl.multiple_of(slot * 64, 64), 64)
        norm_slot(slot)
        value = normed[at_rows, :]
        keys = jnp.dot(value, wk[...], preferred_element_type=F32)
        kv[c, j, x, z, :, 128:256] = jnp.dot(value, wv[...], preferred_element_type=F32).astype(BF)
        kv[c, j, x, z, :, 0:128] = half_norm(keys, kg[...])

    for load in loads[:2]:
        load.wait()
    key_slot(0, y)
    m_ref[...] = jnp.full(m_ref.shape, -1e30, F32)
    a_begin(0)
    l_ref[...] = jnp.zeros(l_ref.shape, F32)
    acc[...] = jnp.zeros(acc.shape, F32)
    for d in range(2):
        target, source = ypair[d]
        ref = piece(source, d)
        remote(ref, ref, y1s.at[d, d], y1r.at[d, d], target).wait_recv()
        go(remote(ref, ref, y2s.at[d], y2r.at[d], target))
    for d in range(2):
        target, source = ypair[d]
        ref = piece(source, 1 - d)
        remote(ref, ref, y1s.at[d, 1 - d], y1r.at[d, 1 - d], target).wait_recv()
        key_slot(1 + d, source)
        if d == 0:
            a_begin(1)
            a_x1(0)
        else:
            b_begin(0)
    opposite = lax.rem(y + 2, NT)
    for d in range(2):
        ref = piece(opposite, d)
        remote(ref, ref, y2s.at[d], y2r.at[d], ypair[d][0]).wait_recv()
    key_slot(3, opposite)
    b_begin(1)
    a_x1(1)

    def project_q(n, target):
        queries = dot(wq[:, n * 256 : (n + 1) * 256])
        for k in range(2):
            one = half_norm(queries[:, k * 128 : (k + 1) * 128], qg[2 * n + k : 2 * n + k + 1, :])
            target[:, k * 128 : (k + 1) * 128] = one * jnp.asarray(0.125, BF)

    for load in loads[2:5]:
        load.wait()
    project_q(1, q_far)
    q_copy = remote(q_far, q_in, ex_s.at[0], ex_r.at[0], pdev)
    a_x2(0)
    b_z(0, 1)
    b_x1(0, 0)
    go(q_copy)

    def gate(n):
        span = slice(n * 256, (n + 1) * 256)
        gated[:, span] = (dot(wa[:, span]) * jax.nn.sigmoid(dot(wb[:, span]))).astype(BF)

    gate(0)
    a_x2(1)
    dd_send(0, 0)
    gate(1)
    halo_copy = remote(gated.at[pl.ds(224, 32)], halo, ex_s.at[1], ex_r.at[1], nxt)
    b_z(1, 1)
    b_x1(1, 0)
    go(halo_copy)
    project_q(0, q_own)
    b_x2(0, 0)
    b_x1(0, 1)
    low = lax.broadcasted_iota(jnp.int32, (256, 128), 1) < 64

    def pad(which, source):
        for k in range(2):
            head = source[:, k * 128 : (k + 1) * 128].astype(F32)
            qpad[which, 2 * k] = jnp.where(low, head, 0.0).astype(BF)
            qpad[which, 2 * k + 1] = jnp.where(low, 0.0, head).astype(BF)

    pad(0, q_own)
    for k in range(4):
        gpad[k, 32:288, :] = gated[:, k * 128 : (k + 1) * 128].astype(F32)
    b_x2(1, 0)
    dd_send(1, 0)
    halo_copy.wait_recv()
    for k in range(4):
        gpad[k, 0:32, :] = jnp.where(sp > 0, halo[:, k * 128 : (k + 1) * 128].astype(F32), 0.0)

    def conv_step(k, carry):
        one, two = carry
        total = jnp.zeros((256, 128), F32)
        lanes = pl.ds(pl.multiple_of(k * 128, 128), 128)
        for j in range(KW):
            total = total + taps[j : j + 1, lanes] * gpad[k, j + 2 : j + 258, :]
        csum[k] = total
        return one + total, two + total * total

    nothing = jnp.zeros((256, 128), F32)
    one, two = lax.fori_loop(0, 4, conv_step, (nothing, nothing))
    lane = lax.broadcasted_iota(jnp.int32, (256, 128), 1)
    stat_out[...] = jnp.where(
        lane == 0, jnp.sum(one, axis=1, keepdims=True), jnp.sum(two, axis=1, keepdims=True)
    )
    b_x1(1, 1)
    q_copy.wait_recv()
    pad(1, q_in)
    for k in range(3):
        go(remote(stat_out, stat_in.at[k], st_s.at[k], st_r.at[k], ydev[k]))
    attend_first(c)
    events_a(1)
    dd_recv(0)
    attend_first(sib)
    events_b(1)
    for k in range(3):
        remote(stat_out, stat_in.at[k], st_s.at[k], st_r.at[k], ydev[k]).wait_recv()
    total = (stat_out[...] + stat_in[0]) + (stat_in[1] + stat_in[2])
    mean = total[:, 0:1] / (NT * 512)
    mean_sq = total[:, 1:2] / (NT * 512)
    scale = lax.rsqrt(mean_sq - mean * mean + 1e-5)
    for k in range(4):
        span = slice(k * 128, (k + 1) * 128)
        conv_out[:, span] = jax.nn.silu((csum[k] - mean) * scale * ln_gain[:, span]).astype(BF)
    for load in loads[5:]:
        load.wait()
    for n in range(4):
        span = pl.ds(n * 512, 512)
        part[:, span] = jnp.dot(conv_out[...], wc[:, span], preferred_element_type=F32)

    def finish(which, out_ref, log_ref):
        table = jnp.zeros((256, 128), F32)
        for k in range(2):
            outs = []
            for m in range(2):
                total = jnp.sum(l_ref[which, 2 * k + m], axis=1, keepdims=True)
                outs.append(acc[which, 2 * k + m] / total)
                table = jnp.where(lane == 2 * k + m, m_ref[which, 2 * k + m] + jnp.log(total), table)
            row = 2 * which + k
            diff = outs[0] - lam[row] * outs[1]
            scale = lax.rsqrt(jnp.mean(diff * diff, axis=1, keepdims=True) + 1e-6)
            out_ref[:, k * 128 : (k + 1) * 128] = (diff * scale * sub_gain[...]).astype(BF)
        log_ref[...] = table.T[0:8, :]

    back = [
        remote(ret_out, ret_in, ex_s.at[2], ex_r.at[2], pdev),
        remote(log_out, log_in, ex_s.at[3], ex_r.at[3], pdev),
    ]

    def send_back(now):
        @pl.when(now)
        def _():
            finish(1, ret_out, log_out)
            for copy in back:
                copy.start()

    done_by_three = lax.rem(z, 4) >= 2
    for t in range(1, 4):
        events_a(t + 1)
        dd_recv(t)
        attend(t, 0)
        events_b(t + 1)
        attend(t, 1)
    send_back(done_by_three)
    dd_recv(4)
    attend(4, 0, 0, 2)
    send_back(jnp.logical_not(done_by_three))
    attend(4, 0, 2, 4)
    attend_last()
    finish(0, attn, log_self)
    for n in range(4):
        span = pl.ds(n * 512, 512)
        part[:, span] += jnp.dot(attn[...], wo[0:256, span], preferred_element_type=F32)
    for copy in back:
        copy.wait_recv()
    for which, table in ((0, log_self), (1, log_in)):
        for k in range(2):
            for m in range(2):
                logs[m, 2 * which + k : 2 * which + k + 1, :] = table[2 * k + m : 2 * k + m + 1, :]

    targets = (up, down)
    blocks = (lax.rem(y + 1, NT), lax.rem(y + 3, NT))

    def block_rows(block):
        return pl.ds(pl.multiple_of(block * 64, 64), 64)

    for n in range(4):
        span = pl.ds(n * 512, 512)
        part[:, span] += jnp.dot(ret_in[...], wo[256:512, span], preferred_element_type=F32)
        if n % 2 == 1:
            d = n // 2
            wide = pl.ds(d * 1024, 1024)
            far[d] = part[block_rows(opposite), wide].astype(BF)
            near[d] = part[block_rows(blocks[1 - d]), wide].astype(BF)
            go(remote(far.at[d], r1.at[d], o1s.at[d], o1r.at[d], targets[d]))
            go(remote(near.at[d], r2.at[1 - d, d], o2s.at[1 - d, d], o2r.at[1 - d, d], targets[1 - d]))
    for d in range(2):
        remote(far.at[d], r1.at[d], o1s.at[d], o1r.at[d], targets[d]).wait_recv()
        wide = pl.ds(d * 1024, 1024)
        total_out[d] = (part[block_rows(blocks[d]), wide] + r1[d].astype(F32)).astype(BF)
        go(remote(total_out.at[d], r2.at[d, d], o2s.at[d, d], o2r.at[d, d], targets[d]))
    for d in (1, 0):
        for k in (1 - d, d):
            remote(total_out.at[d], r2.at[k, d], o2s.at[k, d], o2r.at[k, d], targets[k]).wait_recv()
        wide = pl.ds(d * 1024, 1024)
        mixed[:, wide] = (part[block_rows(y), wide] + (r2[0, d].astype(F32) + r2[1, d].astype(F32))).astype(BF)
    for copy in [*sends, *back]:
        copy.wait_send()
    all_sent()


def on_device(
    tokens, norm_gain, w_glu_a, w_glu_b, conv_taps, ln_gain, w_query, w_key, w_value,
    query_gain, key_gain, lam_head, sub_gain, w_out_conv, w_out_attn,
):
    dma = pltpu.SemaphoreType.DMA

    def vm(*shape, dtype=BF):
        return pltpu.VMEM(shape, dtype)

    return pl.pallas_call(
        layer_kernel,
        out_shape=(jax.ShapeDtypeStruct((64, 2048), BF), jax.ShapeDtypeStruct((2, 4, 256), F32)),
        in_specs=[VM, VM, HBM, HBM, HBM, HBM, HBM, VM, VM, VM, VM, SM, VM, HBM, HBM],
        out_specs=(VM, VM),
        scratch_shapes=[
            vm(4, 64, 2048), vm(256, 2048),
            vm(2048, 512), vm(2048, 512), vm(2048, 512), vm(2048, 128), vm(2048, 128),
            vm(512, 2048), vm(512, 2048),
            vm(256, 512), vm(256, 256), vm(256, 256),
            vm(2, 4, NX, NZ, 64, 256), vm(256, 256), vm(2, 4, 256, 128),
            vm(2, 4, 256, 128, dtype=F32), vm(2, 4, 256, 128, dtype=F32), vm(2, 4, 256, 128, dtype=F32),
            vm(32, 512), vm(4, 288, 128, dtype=F32), vm(4, 256, 128, dtype=F32),
            vm(256, 128, dtype=F32), vm(3, 256, 128, dtype=F32),
            vm(256, 256), vm(256, 512), vm(256, 256), vm(256, 256),
            vm(8, 256, dtype=F32), vm(8, 256, dtype=F32), vm(8, 256, dtype=F32),
            vm(256, 2048, dtype=F32), vm(2, 64, 1024), vm(2, 64, 1024), vm(2, 64, 1024), vm(2, 64, 1024),
            vm(2, 2, 64, 1024),
            dma((7,)), dma, dma((2, 2)), dma((2, 2)), dma((2,)), dma((2,)),
            dma, dma((2, 2)),
            dma, dma((2, 4, 2)),
            dma, dma((2, 4, 2)),
            dma, dma((2, 5, 2, 2)),
            dma, dma((5, 2)),
            dma((4,)), dma((4,)),
            dma((3,)), dma((3,)),
            dma((2,)), dma((2,)), dma((2, 2)), dma((2, 2)),
        ],
        compiler_params=pltpu.CompilerParams(
            collective_id=0, has_side_effects=True, vmem_limit_bytes=60 * 1024 * 1024
        ),
        name="layer",
    )(
        tokens, norm_gain.reshape(1, -1), w_glu_a, w_glu_b, w_query, w_key, w_value, query_gain, key_gain,
        conv_taps, ln_gain.reshape(1, -1), lam_head, sub_gain.reshape(1, -1), w_out_conv, w_out_attn,
    )


def solution(mesh):
    return jax.shard_map(
        on_device,
        mesh=mesh,
        in_specs=(
            P(("sp", "tp"), None), P(), P(None, "tp"), P(None, "tp"), P(None, "tp"), P("tp"),
            P(None, "tp"), P(None, "tp"), P(None, "tp"), P("tp", None), P("tp", None), P("tp"),
            P(), P("tp", None), P("tp", None),
        ),
        out_specs=(P(("sp", "tp"), None), P(None, "tp", "sp")),
        check_vma=False,
    )
```

```python
import functools

import jax
import jax.numpy as jnp
from jax import lax
from jax.experimental import pallas as pl
from jax.experimental.pallas import tpu as pltpu
from jax.sharding import PartitionSpec as P

KW = 31
MESH = pl.DeviceIdType.MESH
NZ, NX, NT = 8, 4, 4
BF, F32 = jnp.bfloat16, jnp.float32
VM = pl.BlockSpec(memory_space=pltpu.VMEM)


def remote(src, dst, send, recv, device):
    return pltpu.make_async_remote_copy(
        src_ref=src, dst_ref=dst, send_sem=send, recv_sem=recv, device_id=device, device_id_type=MESH
    )


def greet(devices):
    barrier = pltpu.get_barrier_semaphore()
    for device in devices:
        pl.semaphore_signal(barrier, inc=1, device_id=device, device_id_type=MESH)
    return lambda: pl.semaphore_wait(barrier, len(devices))


def half_norm(value, gain):
    low = lax.broadcasted_iota(jnp.int32, value.shape, 1) < 64
    squares = value * value
    first = jnp.sum(jnp.where(low, squares, 0.0), axis=1, keepdims=True)
    second = jnp.sum(jnp.where(low, 0.0, squares), axis=1, keepdims=True)
    scale = jnp.where(low, lax.rsqrt(first / 64 + 1e-6), lax.rsqrt(second / 64 + 1e-6))
    return (value * scale * gain).astype(BF)


HBM = pl.BlockSpec(memory_space=pltpu.MemorySpace.HBM)
SM = pl.BlockSpec(memory_space=pltpu.SMEM)


def layer_kernel(
    tok, gain, wa_h, wb_h, wq_h, wk_h, wv_h, qg, kg, taps, ln_gain, lam, sub_gain, wc_h, wo_h,
    mixed, logs,
    rows, normed, wa, wb, wq, wk, wv, wc, wo, gated, q_own, q_far,
    kv, q_in, qpad, m_ref, l_ref, acc, halo, gpad, csum, stat_out, stat_in,
    attn, conv_out, ret_out, ret_in, log_out, log_in, log_self,
    part, far, near, total_out, r1, r2,
    w_sem, own_sem, y1s, y1r, y2s, y2r,
    ax_s, ax_r, az_s, az_r, bz_s, bz_r, bx_s, bx_r, dd_s, dd_r, ex_s, ex_r, st_s, st_r,
    o1s, o1r, o2s, o2r,
):
    sp, y = lax.axis_index("sp"), lax.axis_index("tp")
    z, x, c = sp // 8, lax.rem(sp // 2, 4), lax.rem(sp, 2)
    sib = 1 - c

    def zm(value):
        return lax.rem(value + 2 * NZ, NZ)

    def xm(value):
        return lax.rem(value + 2 * NX, NX)

    def at(zz, xx, cc):
        return {"sp": zz * 8 + xx * 2 + cc, "tp": y}

    zdev = (at(zm(z + 1), x, c), at(zm(z - 1), x, c))
    xdev = (at(z, xm(x + 1), c), at(z, xm(x - 1), c))
    sdev = at(z, x, sib)
    far_z = NZ - 1 - z
    pdev = at(far_z, x, c)
    nxt = {"sp": lax.rem(sp + 1, 64), "tp": y}
    prv = {"sp": lax.rem(sp + 63, 64), "tp": y}
    ydev = [{"sp": sp, "tp": lax.rem(y + k, NT)} for k in (1, 2, 3)]
    up, down = ydev[0], ydev[2]
    meet = greet([*zdev, *xdev, sdev, pdev, nxt, prv, *ydev])
    sends = []

    def go(copy, keep=True):
        copy.start()
        if keep:
            sends.append(copy)

    def origin(s, d):
        return zm(z - s) if d == 0 else zm(z + s)

    def signs(s):
        return (0, 1) if 0 < s < 4 else (0,)

    def ways(s, i):
        return (0, 1) if s < 4 else (i,)

    offsets = (0, -1, 1, 2)

    def ax1(a, d):
        ref = kv.at[c, a, x, z]
        go(remote(ref, ref, ax_s, ax_r.at[a, 0], xdev[d]), False)

    def ax2(a):
        ref = kv.at[c, a, xm(x - 1 + 2 * a), z]
        go(remote(ref, ref, ax_s, ax_r.at[a, 1], xdev[a]), False)

    def az(a, s, d, j):
        ref = kv.at[c, a, xm(x + offsets[j]) if s == 1 else slice(None), origin(s - 1, d)]
        go(remote(ref, ref, az_s, az_r.at[a, s - 1, d], zdev[d]), False)

    def bz(i, s, d, landing):
        ref = kv.at[c, 2 + i, x, origin(s if landing else s - 1, d)]
        return remote(ref, ref, bz_s, bz_r.at[i, s - 1, d], zdev[d])

    def bx1(i, s, g, d):
        ref = kv.at[c, 2 + i, x, origin(s, g)]
        go(remote(ref, ref, bx_s, bx_r.at[i, s, g, 0], xdev[d]), False)

    def bx2(i, s, g, landing):
        ref = kv.at[c, 2 + i, xm(x + 2) if landing else xm(x - 1 + 2 * i), origin(s, g)]
        return remote(ref, ref, bx_s, bx_r.at[i, s, g, 1], xdev[i])

    def taken(ref, send, recv):
        remote(ref, ref, send, recv, sdev).wait_recv()

    def a_begin(a):
        for d in range(2):
            ax1(a, d)
        for d in range(2):
            az(a, 1, d, 0)

    def a_x1(a):
        taken(kv.at[c, a, pl.ds(0, 2), z], ax_s, ax_r.at[a, 0])
        ax2(a)
        for j in (1, 2):
            for d in range(2):
                az(a, 1, d, j)

    def a_x2(a):
        taken(kv.at[c, a, 0, z], ax_s, ax_r.at[a, 1])
        for d in range(2):
            az(a, 1, d, 3)

    def a_z(a, s):
        for d in ways(s, a):
            taken(kv.at[c, a, :, origin(s, d)], az_s, az_r.at[a, s - 1, d])
            if s < 3 or (s == 3 and d == a):
                az(a, s + 1, d, 0)

    def b_begin(i):
        for d in range(2):
            go(bz(i, 1, d, False), False)
        for d in range(2):
            bx1(i, 0, 0, d)

    def b_z(i, s):
        for d in ways(s, i):
            bz(i, s, d, True).wait_recv()
            if s < 3 or (s == 3 and d == i):
                go(bz(i, s + 1, d, False), False)
            for way in range(2):
                bx1(i, s, d if s < 4 else 0, way)

    def b_x1(i, s):
        for g in signs(s):
            taken(kv.at[c, 2 + i, pl.ds(0, 2), origin(s, g)], bx_s, bx_r.at[i, s, g, 0])
            go(bx2(i, s, g, False), False)

    def b_x2(i, s):
        for g in signs(s):
            bx2(i, s, g, True).wait_recv()

    def dd_send(h, s):
        for g in signs(s):
            ref = kv.at[c, pl.ds(2 * h, 2), :, origin(s, g)]
            go(remote(ref, ref, dd_s, dd_r.at[s, g], sdev), False)

    def dd_recv(s):
        for g in signs(s):
            taken(kv.at[sib, :, :, origin(s, g)], dd_s, dd_r.at[s, g])

    def all_sent():
        for ref, sem in (
            (kv.at[c, pl.ds(0, 3), pl.ds(0, 2), 0], ax_s),
            (kv.at[c, pl.ds(0, 2), :, pl.ds(0, 7)], az_s),
            (kv.at[c, pl.ds(0, 2), 0, pl.ds(0, 7)], bz_s),
            (kv.at[c, :, :, pl.ds(0, 3)], bx_s),
            (kv.at[c], dd_s),
        ):
            remote(ref, ref, sem, ax_r.at[0, 0], sdev).wait_send()

    slot_rows = [lax.rem(y + k, NT) for k in (0, 3, 1, 2)]

    def tile(which, cc, zt, masked):
        pieces = [(j, k) for j in range(4) for k in range(NX)]
        keys = jnp.concatenate([kv[cc, j, k, zt, :, 0:128] for j, k in pieces], axis=0)
        values = jnp.concatenate([kv[cc, j, k, zt, :, 128:256] for j, k in pieces], axis=0)
        if masked:
            row = lax.broadcasted_iota(jnp.int32, (256, 128), 0) + (x * 512 + c * 256)
            col = lax.broadcasted_iota(jnp.int32, (256, 128), 1)
            col = jnp.where(col < 64, col, col + 448) + cc * 256
        scores = [
            lax.dot_general(
                qpad[which, pl.ds(2 * n, 2)].reshape(512, 128),
                keys,
                (((1,), (1,)), ((), ())),
                preferred_element_type=F32,
            )
            for n in range(2)
        ]
        for n in range(2):
            weights, fades = [], []
            for k in range(2):
                hm = 2 * n + k
                parts = [scores[n][k * 256 : (k + 1) * 256, p * 128 : (p + 1) * 128] for p in range(8)]
                if masked:
                    parts = [
                        jnp.where(col + ((p % 2) * 1024 + slot_rows[p // 2] * 64) <= row, item, -1e30)
                        for p, item in enumerate(parts)
                    ]
                old = m_ref[which, hm]
                new = jnp.maximum(old, jnp.max(functools.reduce(jnp.maximum, parts), axis=1, keepdims=True))
                fade = jnp.exp(old - new)
                parts = [jnp.exp(item - new) for item in parts]
                m_ref[which, hm] = new
                l_ref[which, hm] = l_ref[which, hm] * fade + functools.reduce(jnp.add, parts)
                weights.append(jnp.concatenate([item.astype(BF) for item in parts], axis=1))
                fades.append(fade)
            outs = jnp.dot(jnp.concatenate(weights, axis=0), values, preferred_element_type=F32)
            for k in range(2):
                hm = 2 * n + k
                acc[which, hm] = acc[which, hm] * fades[k] + outs[k * 256 : (k + 1) * 256]

    early = z < NZ // 2

    def attend(s, g, first=0, last=4):
        zt = zm(z - s + 2 * s * g)

        def step(i, carry):
            which = 1 - i // 2
            cc = lax.rem(c + i, 2)
            zq = jnp.where(which == 0, z, far_z)

            @pl.when(zt < zq)
            def _():
                tile(which, cc, zt, False)

            if s in (1, 3):

                @pl.when(zt == zq)
                def _():
                    tile(which, cc, zt, True)

            return carry

        lax.fori_loop(first, last, step, 0)

    def attend_first(cc):
        @pl.when(early)
        def _():
            tile(1, cc, z, False)

        @pl.when(jnp.logical_not(early))
        def _():
            tile(0, cc, z, True)

    def attend_last():
        def step(cc, carry):
            @pl.when(early)
            def _():
                tile(0, cc, z, True)

            return carry

        lax.fori_loop(0, 2, step, 0)

    def events_a(t):
        if t + 1 <= 4:
            for i in range(2):
                b_z(i, t + 1)
        a_z(0, t)

    def events_b(t):
        a_z(1, t)
        dd_send(0, t)
        if t + 1 <= 4:
            for i in range(2):
                b_x1(i, t + 1)
        for i in range(2):
            b_x2(i, t)
        dd_send(1, t)

    pairs = ((wk_h, wk), (wv_h, wv), (wq_h, wq), (wa_h, wa), (wb_h, wb), (wc_h, wc), (wo_h, wo))
    loads = [pltpu.make_async_copy(src, dst, w_sem.at[i]) for i, (src, dst) in enumerate(pairs)]
    own_rows = pltpu.make_async_copy(tok, rows.at[y], own_sem)
    own_rows.start()
    for load in loads[:2]:
        load.start()
    meet()

    def piece(slot, half):
        return rows.at[slot, pl.ds(half * 32, 32)]

    ypair = ((up, lax.rem(y + 3, NT)), (down, lax.rem(y + 1, NT)))
    for order in range(2):
        for d in range(2):
            half = order if d == 0 else 1 - order
            go(remote(tok.at[pl.ds(half * 32, 32)], piece(y, half), y1s.at[d, half], y1r.at[d, half], ypair[d][0]))
    for load in loads[2:]:
        load.start()
    own_rows.wait()

    def norm_slot(slot):
        value = rows[slot].astype(F32)
        scale = lax.rsqrt(jnp.mean(value * value, axis=1, keepdims=True) + 1e-6)
        normed[pl.ds(pl.multiple_of(slot * 64, 64), 64), :] = (value * scale * gain[...]).astype(BF)

    def dot(weight):
        return jnp.dot(normed[...], weight, preferred_element_type=F32)

    def key_slot(j, slot):
        at_rows = pl.ds(pl.multiple_of(slot * 64, 64), 64)
        norm_slot(slot)
        value = normed[at_rows, :]
        keys = jnp.dot(value, wk[...], preferred_element_type=F32)
        kv[c, j, x, z, :, 128:256] = jnp.dot(value, wv[...], preferred_element_type=F32).astype(BF)
        kv[c, j, x, z, :, 0:128] = half_norm(keys, kg[...])

    for load in loads[:2]:
        load.wait()
    key_slot(0, y)
    m_ref[...] = jnp.full(m_ref.shape, -1e30, F32)
    a_begin(0)
    l_ref[...] = jnp.zeros(l_ref.shape, F32)
    acc[...] = jnp.zeros(acc.shape, F32)
    for d in range(2):
        target, source = ypair[d]
        ref = piece(source, d)
        remote(ref, ref, y1s.at[d, d], y1r.at[d, d], target).wait_recv()
        go(remote(ref, ref, y2s.at[d], y2r.at[d], target))
    for d in range(2):
        target, source = ypair[d]
        ref = piece(source, 1 - d)
        remote(ref, ref, y1s.at[d, 1 - d], y1r.at[d, 1 - d], target).wait_recv()
        key_slot(1 + d, source)
        if d == 0:
            a_begin(1)
            a_x1(0)
        else:
            b_begin(0)
    opposite = lax.rem(y + 2, NT)
    for d in range(2):
        ref = piece(opposite, d)
        remote(ref, ref, y2s.at[d], y2r.at[d], ypair[d][0]).wait_recv()
    key_slot(3, opposite)
    b_begin(1)

    def project_q(n, target):
        queries = dot(wq[:, n * 256 : (n + 1) * 256])
        for k in range(2):
            one = half_norm(queries[:, k * 128 : (k + 1) * 128], qg[2 * n + k : 2 * n + k + 1, :])
            target[:, k * 128 : (k + 1) * 128] = one * jnp.asarray(0.125, BF)

    for load in loads[2:5]:
        load.wait()
    project_q(1, q_far)
    q_copy = remote(q_far, q_in, ex_s.at[0], ex_r.at[0], pdev)
    a_x1(1)
    a_x2(0)

    def gate(n):
        span = slice(n * 256, (n + 1) * 256)
        gated[:, span] = (dot(wa[:, span]) * jax.nn.sigmoid(dot(wb[:, span]))).astype(BF)

    gate(0)
    go(q_copy)
    b_z(0, 1)
    b_x1(0, 0)
    gate(1)
    a_x2(1)
    dd_send(0, 0)
    project_q(0, q_own)
    halo_copy = remote(gated.at[pl.ds(224, 32)], halo, ex_s.at[1], ex_r.at[1], nxt)
    go(halo_copy)
    b_z(1, 1)
    b_x1(1, 0)
    b_x2(0, 0)
    b_x1(0, 1)
    low = lax.broadcasted_iota(jnp.int32, (256, 128), 1) < 64

    def pad(which, source):
        for k in range(2):
            head = source[:, k * 128 : (k + 1) * 128].astype(F32)
            qpad[which, 2 * k] = jnp.where(low, head, 0.0).astype(BF)
            qpad[which, 2 * k + 1] = jnp.where(low, 0.0, head).astype(BF)

    pad(0, q_own)
    b_x2(1, 0)
    dd_send(1, 0)
    q_copy.wait_recv()
    pad(1, q_in)
    attend_first(c)
    b_x1(1, 1)
    events_a(1)
    dd_recv(0)
    attend_first(sib)
    for k in range(4):
        gpad[k, 32:288, :] = gated[:, k * 128 : (k + 1) * 128].astype(F32)
    halo_copy.wait_recv()
    for k in range(4):
        gpad[k, 0:32, :] = jnp.where(sp > 0, halo[:, k * 128 : (k + 1) * 128].astype(F32), 0.0)

    def conv_step(k, carry):
        one, two = carry
        total = jnp.zeros((256, 128), F32)
        lanes = pl.ds(pl.multiple_of(k * 128, 128), 128)
        for j in range(KW):
            total = total + taps[j : j + 1, lanes] * gpad[k, j + 2 : j + 258, :]
        csum[k] = total
        return one + total, two + total * total

    nothing = jnp.zeros((256, 128), F32)
    one, two = lax.fori_loop(0, 4, conv_step, (nothing, nothing))
    lane = lax.broadcasted_iota(jnp.int32, (256, 128), 1)
    stat_out[...] = jnp.where(
        lane == 0, jnp.sum(one, axis=1, keepdims=True), jnp.sum(two, axis=1, keepdims=True)
    )
    for k in range(3):
        go(remote(stat_out, stat_in.at[k], st_s.at[k], st_r.at[k], ydev[k]))
    events_b(1)

    def finish(which, out_ref, log_ref):
        table = jnp.zeros((256, 128), F32)
        for k in range(2):
            outs = []
            for m in range(2):
                total = jnp.sum(l_ref[which, 2 * k + m], axis=1, keepdims=True)
                outs.append(acc[which, 2 * k + m] / total)
                table = jnp.where(lane == 2 * k + m, m_ref[which, 2 * k + m] + jnp.log(total), table)
            row = 2 * which + k
            diff = outs[0] - lam[row] * outs[1]
            scale = lax.rsqrt(jnp.mean(diff * diff, axis=1, keepdims=True) + 1e-6)
            out_ref[:, k * 128 : (k + 1) * 128] = (diff * scale * sub_gain[...]).astype(BF)
        log_ref[...] = table.T[0:8, :]

    back = [
        remote(ret_out, ret_in, ex_s.at[2], ex_r.at[2], pdev),
        remote(log_out, log_in, ex_s.at[3], ex_r.at[3], pdev),
    ]

    def send_back(now):
        @pl.when(now)
        def _():
            finish(1, ret_out, log_out)
            for copy in back:
                copy.start()

    done_by_three = lax.rem(z, 4) >= 2
    def close_conv():
        for k in range(3):
            remote(stat_out, stat_in.at[k], st_s.at[k], st_r.at[k], ydev[k]).wait_recv()
        total = (stat_out[...] + stat_in[0]) + (stat_in[1] + stat_in[2])
        mean = total[:, 0:1] / (NT * 512)
        mean_sq = total[:, 1:2] / (NT * 512)
        scale = lax.rsqrt(mean_sq - mean * mean + 1e-5)
        for k in range(4):
            span = slice(k * 128, (k + 1) * 128)
            conv_out[:, span] = jax.nn.silu((csum[k] - mean) * scale * ln_gain[:, span]).astype(BF)
        for load in loads[5:]:
            load.wait()
        for n in range(4):
            span = pl.ds(n * 512, 512)
            part[:, span] = jnp.dot(conv_out[...], wc[:, span], preferred_element_type=F32)

    for t in range(1, 4):
        events_a(t + 1)
        dd_recv(t)
        attend(t, 0)
        events_b(t + 1)
        attend(t, 1)
        if t == 1:
            close_conv()
    send_back(done_by_three)
    dd_recv(4)
    attend(4, 0, 0, 2)
    send_back(jnp.logical_not(done_by_three))
    attend(4, 0, 2, 4)
    attend_last()
    finish(0, attn, log_self)
    for n in range(4):
        span = pl.ds(n * 512, 512)
        part[:, span] += jnp.dot(attn[...], wo[0:256, span], preferred_element_type=F32)
    for copy in back:
        copy.wait_recv()
    for which, table in ((0, log_self), (1, log_in)):
        for k in range(2):
            for m in range(2):
                logs[m, 2 * which + k : 2 * which + k + 1, :] = table[2 * k + m : 2 * k + m + 1, :]

    targets = (up, down)
    blocks = (lax.rem(y + 1, NT), lax.rem(y + 3, NT))

    def block_rows(block):
        return pl.ds(pl.multiple_of(block * 64, 64), 64)

    for n in range(4):
        span = pl.ds(n * 512, 512)
        part[:, span] += jnp.dot(ret_in[...], wo[256:512, span], preferred_element_type=F32)
        if n % 2 == 1:
            d = n // 2
            wide = pl.ds(d * 1024, 1024)
            far[d] = part[block_rows(opposite), wide].astype(BF)
            near[d] = part[block_rows(blocks[1 - d]), wide].astype(BF)
            go(remote(far.at[d], r1.at[d], o1s.at[d], o1r.at[d], targets[d]))
            go(remote(near.at[d], r2.at[1 - d, d], o2s.at[1 - d, d], o2r.at[1 - d, d], targets[1 - d]))
    for d in range(2):
        remote(far.at[d], r1.at[d], o1s.at[d], o1r.at[d], targets[d]).wait_recv()
        wide = pl.ds(d * 1024, 1024)
        total_out[d] = (part[block_rows(blocks[d]), wide] + r1[d].astype(F32)).astype(BF)
        go(remote(total_out.at[d], r2.at[d, d], o2s.at[d, d], o2r.at[d, d], targets[d]))
    for d in (1, 0):
        for k in (1 - d, d):
            remote(total_out.at[d], r2.at[k, d], o2s.at[k, d], o2r.at[k, d], targets[k]).wait_recv()
        wide = pl.ds(d * 1024, 1024)
        mixed[:, wide] = (part[block_rows(y), wide] + (r2[0, d].astype(F32) + r2[1, d].astype(F32))).astype(BF)
    for copy in [*sends, *back]:
        copy.wait_send()
    all_sent()


def on_device(
    tokens, norm_gain, w_glu_a, w_glu_b, conv_taps, ln_gain, w_query, w_key, w_value,
    query_gain, key_gain, lam_head, sub_gain, w_out_conv, w_out_attn,
):
    dma = pltpu.SemaphoreType.DMA

    def vm(*shape, dtype=BF):
        return pltpu.VMEM(shape, dtype)

    return pl.pallas_call(
        layer_kernel,
        out_shape=(jax.ShapeDtypeStruct((64, 2048), BF), jax.ShapeDtypeStruct((2, 4, 256), F32)),
        in_specs=[VM, VM, HBM, HBM, HBM, HBM, HBM, VM, VM, VM, VM, SM, VM, HBM, HBM],
        out_specs=(VM, VM),
        scratch_shapes=[
            vm(4, 64, 2048), vm(256, 2048),
            vm(2048, 512), vm(2048, 512), vm(2048, 512), vm(2048, 128), vm(2048, 128),
            vm(512, 2048), vm(512, 2048),
            vm(256, 512), vm(256, 256), vm(256, 256),
            vm(2, 4, NX, NZ, 64, 256), vm(256, 256), vm(2, 4, 256, 128),
            vm(2, 4, 256, 128, dtype=F32), vm(2, 4, 256, 128, dtype=F32), vm(2, 4, 256, 128, dtype=F32),
            vm(32, 512), vm(4, 288, 128, dtype=F32), vm(4, 256, 128, dtype=F32),
            vm(256, 128, dtype=F32), vm(3, 256, 128, dtype=F32),
            vm(256, 256), vm(256, 512), vm(256, 256), vm(256, 256),
            vm(8, 256, dtype=F32), vm(8, 256, dtype=F32), vm(8, 256, dtype=F32),
            vm(256, 2048, dtype=F32), vm(2, 64, 1024), vm(2, 64, 1024), vm(2, 64, 1024), vm(2, 64, 1024),
            vm(2, 2, 64, 1024),
            dma((7,)), dma, dma((2, 2)), dma((2, 2)), dma((2,)), dma((2,)),
            dma, dma((2, 2)),
            dma, dma((2, 4, 2)),
            dma, dma((2, 4, 2)),
            dma, dma((2, 5, 2, 2)),
            dma, dma((5, 2)),
            dma((4,)), dma((4,)),
            dma((3,)), dma((3,)),
            dma((2,)), dma((2,)), dma((2, 2)), dma((2, 2)),
        ],
        compiler_params=pltpu.CompilerParams(
            collective_id=0, has_side_effects=True, vmem_limit_bytes=60 * 1024 * 1024
        ),
        name="layer",
    )(
        tokens, norm_gain.reshape(1, -1), w_glu_a, w_glu_b, w_query, w_key, w_value, query_gain, key_gain,
        conv_taps, ln_gain.reshape(1, -1), lam_head, sub_gain.reshape(1, -1), w_out_conv, w_out_attn,
    )


def solution(mesh):
    return jax.shard_map(
        on_device,
        mesh=mesh,
        in_specs=(
            P(("sp", "tp"), None), P(), P(None, "tp"), P(None, "tp"), P(None, "tp"), P("tp"),
            P(None, "tp"), P(None, "tp"), P(None, "tp"), P("tp", None), P("tp", None), P("tp"),
            P(), P("tp", None), P("tp", None),
        ),
        out_specs=(P(("sp", "tp"), None), P(None, "tp", "sp")),
        check_vma=False,
    )
```

```python
import functools

import jax
import jax.numpy as jnp
from jax import lax
from jax.experimental import pallas as pl
from jax.experimental.pallas import tpu as pltpu
from jax.sharding import PartitionSpec as P

KW = 31
MESH = pl.DeviceIdType.MESH
NZ, NX, NT = 8, 4, 4
BF, F32 = jnp.bfloat16, jnp.float32
VM = pl.BlockSpec(memory_space=pltpu.VMEM)


def remote(src, dst, send, recv, device):
    return pltpu.make_async_remote_copy(
        src_ref=src, dst_ref=dst, send_sem=send, recv_sem=recv, device_id=device, device_id_type=MESH
    )


def greet(devices):
    barrier = pltpu.get_barrier_semaphore()
    for device in devices:
        pl.semaphore_signal(barrier, inc=1, device_id=device, device_id_type=MESH)
    return lambda: pl.semaphore_wait(barrier, len(devices))


def half_norm(value, gain):
    low = lax.broadcasted_iota(jnp.int32, value.shape, 1) < 64
    squares = value * value
    first = jnp.sum(jnp.where(low, squares, 0.0), axis=1, keepdims=True)
    second = jnp.sum(jnp.where(low, 0.0, squares), axis=1, keepdims=True)
    scale = jnp.where(low, lax.rsqrt(first / 64 + 1e-6), lax.rsqrt(second / 64 + 1e-6))
    return (value * scale * gain).astype(BF)


HBM = pl.BlockSpec(memory_space=pltpu.MemorySpace.HBM)
SM = pl.BlockSpec(memory_space=pltpu.SMEM)


def layer_kernel(
    tok, gain, wa_h, wb_h, wq_h, wk_h, wv_h, qg, kg, taps, ln_gain, lam, sub_gain, wc_h, wo_h,
    mixed, logs,
    rows, normed, wa, wb, wq, wk, wv, wc, wo, gated, q_own, q_far,
    kv, q_in, qpad, m_ref, l_ref, acc, halo, gpad, csum, stat_out, stat_in,
    attn, conv_out, ret_out, ret_in, log_out, log_in, log_self,
    part, far, near, total_out, r1, r2,
    w_sem, own_sem, y1s, y1r, y2s, y2r,
    ax_s, ax_r, az_s, az_r, bz_s, bz_r, bx_s, bx_r, dd_s, dd_r, ex_s, ex_r, st_s, st_r,
    o1s, o1r, o2s, o2r,
):
    sp, y = lax.axis_index("sp"), lax.axis_index("tp")
    z, x, c = sp // 8, lax.rem(sp // 2, 4), lax.rem(sp, 2)
    sib = 1 - c

    def zm(value):
        return lax.rem(value + 2 * NZ, NZ)

    def xm(value):
        return lax.rem(value + 2 * NX, NX)

    def at(zz, xx, cc):
        return {"sp": zz * 8 + xx * 2 + cc, "tp": y}

    zdev = (at(zm(z + 1), x, c), at(zm(z - 1), x, c))
    xdev = (at(z, xm(x + 1), c), at(z, xm(x - 1), c))
    sdev = at(z, x, sib)
    far_z = NZ - 1 - z
    pdev = at(far_z, x, c)
    nxt = {"sp": lax.rem(sp + 1, 64), "tp": y}
    prv = {"sp": lax.rem(sp + 63, 64), "tp": y}
    ydev = [{"sp": sp, "tp": lax.rem(y + k, NT)} for k in (1, 2, 3)]
    up, down = ydev[0], ydev[2]
    meet = greet([*zdev, *xdev, sdev, pdev, nxt, prv, *ydev])
    sends = []

    def go(copy, keep=True):
        copy.start()
        if keep:
            sends.append(copy)

    def origin(s, d):
        return zm(z - s) if d == 0 else zm(z + s)

    def signs(s):
        return (0, 1) if 0 < s < 4 else (0,)

    def ways(s, i):
        return (0, 1) if s < 4 else (i,)

    offsets = (0, -1, 1, 2)

    def ax1(a, d):
        ref = kv.at[c, a, x, z]
        go(remote(ref, ref, ax_s, ax_r.at[a, 0], xdev[d]), False)

    def ax2(a):
        ref = kv.at[c, a, xm(x - 1 + 2 * a), z]
        go(remote(ref, ref, ax_s, ax_r.at[a, 1], xdev[a]), False)

    def az(a, s, d, j):
        ref = kv.at[c, a, xm(x + offsets[j]) if s == 1 else slice(None), origin(s - 1, d)]
        go(remote(ref, ref, az_s, az_r.at[a, s - 1, d], zdev[d]), False)

    def bz(i, s, d, landing):
        ref = kv.at[c, 2 + i, x, origin(s if landing else s - 1, d)]
        return remote(ref, ref, bz_s, bz_r.at[i, s - 1, d], zdev[d])

    def bx1(i, s, g, d):
        ref = kv.at[c, 2 + i, x, origin(s, g)]
        go(remote(ref, ref, bx_s, bx_r.at[i, s, g, 0], xdev[d]), False)

    def bx2(i, s, g, landing):
        ref = kv.at[c, 2 + i, xm(x + 2) if landing else xm(x - 1 + 2 * i), origin(s, g)]
        return remote(ref, ref, bx_s, bx_r.at[i, s, g, 1], xdev[i])

    def taken(ref, send, recv):
        remote(ref, ref, send, recv, sdev).wait_recv()

    def a_begin(a):
        for d in range(2):
            ax1(a, d)
        for d in range(2):
            az(a, 1, d, 0)

    def a_x1(a):
        taken(kv.at[c, a, pl.ds(0, 2), z], ax_s, ax_r.at[a, 0])
        ax2(a)
        for j in (1, 2):
            for d in range(2):
                az(a, 1, d, j)

    def a_x2(a):
        taken(kv.at[c, a, 0, z], ax_s, ax_r.at[a, 1])
        for d in range(2):
            az(a, 1, d, 3)

    def a_z(a, s):
        for d in ways(s, a):
            taken(kv.at[c, a, :, origin(s, d)], az_s, az_r.at[a, s - 1, d])
            if s < 3 or (s == 3 and d == a):
                az(a, s + 1, d, 0)

    def b_begin(i):
        for d in range(2):
            go(bz(i, 1, d, False), False)
        for d in range(2):
            bx1(i, 0, 0, d)

    def b_z(i, s):
        for d in ways(s, i):
            bz(i, s, d, True).wait_recv()
            if s < 3 or (s == 3 and d == i):
                go(bz(i, s + 1, d, False), False)
            for way in range(2):
                bx1(i, s, d if s < 4 else 0, way)

    def b_x1(i, s):
        for g in signs(s):
            taken(kv.at[c, 2 + i, pl.ds(0, 2), origin(s, g)], bx_s, bx_r.at[i, s, g, 0])
            go(bx2(i, s, g, False), False)

    def b_x2(i, s):
        for g in signs(s):
            bx2(i, s, g, True).wait_recv()

    def dd_send(h, s):
        for g in signs(s):
            ref = kv.at[c, pl.ds(2 * h, 2), :, origin(s, g)]
            go(remote(ref, ref, dd_s, dd_r.at[s, g], sdev), False)

    def dd_recv(s):
        for g in signs(s):
            taken(kv.at[sib, :, :, origin(s, g)], dd_s, dd_r.at[s, g])

    def all_sent():
        for ref, sem in (
            (kv.at[c, pl.ds(0, 3), pl.ds(0, 2), 0], ax_s),
            (kv.at[c, pl.ds(0, 2), :, pl.ds(0, 7)], az_s),
            (kv.at[c, pl.ds(0, 2), 0, pl.ds(0, 7)], bz_s),
            (kv.at[c, :, :, pl.ds(0, 3)], bx_s),
            (kv.at[c], dd_s),
        ):
            remote(ref, ref, sem, ax_r.at[0, 0], sdev).wait_send()

    slot_rows = [lax.rem(y + k, NT) for k in (0, 3, 1, 2)]

    def tile(which, cc, zt, masked):
        pieces = [(j, k) for j in range(4) for k in range(NX)]
        keys = jnp.concatenate([kv[cc, j, k, zt, :, 0:128] for j, k in pieces], axis=0)
        values = jnp.concatenate([kv[cc, j, k, zt, :, 128:256] for j, k in pieces], axis=0)
        if masked:
            row = lax.broadcasted_iota(jnp.int32, (256, 128), 0) + (x * 512 + c * 256)
            col = lax.broadcasted_iota(jnp.int32, (256, 128), 1)
            col = jnp.where(col < 64, col, col + 448) + cc * 256
        scores = [
            lax.dot_general(
                qpad[which, pl.ds(2 * n, 2)].reshape(512, 128),
                keys,
                (((1,), (1,)), ((), ())),
                preferred_element_type=F32,
            )
            for n in range(2)
        ]
        for n in range(2):
            weights, fades = [], []
            for k in range(2):
                hm = 2 * n + k
                parts = [scores[n][k * 256 : (k + 1) * 256, p * 128 : (p + 1) * 128] for p in range(8)]
                if masked:
                    parts = [
                        jnp.where(col + ((p % 2) * 1024 + slot_rows[p // 2] * 64) <= row, item, -1e30)
                        for p, item in enumerate(parts)
                    ]
                old = m_ref[which, hm]
                new = jnp.maximum(old, jnp.max(functools.reduce(jnp.maximum, parts), axis=1, keepdims=True))
                fade = jnp.exp(old - new)
                parts = [jnp.exp(item - new) for item in parts]
                m_ref[which, hm] = new
                l_ref[which, hm] = l_ref[which, hm] * fade + functools.reduce(jnp.add, parts)
                weights.append(jnp.concatenate([item.astype(BF) for item in parts], axis=1))
                fades.append(fade)
            outs = jnp.dot(jnp.concatenate(weights, axis=0), values, preferred_element_type=F32)
            for k in range(2):
                hm = 2 * n + k
                acc[which, hm] = acc[which, hm] * fades[k] + outs[k * 256 : (k + 1) * 256]

    early = z < NZ // 2

    def attend(s, g, first=0, last=4):
        zt = zm(z - s + 2 * s * g)

        def step(i, carry):
            which = 1 - i // 2
            cc = lax.rem(c + i, 2)
            zq = jnp.where(which == 0, z, far_z)

            @pl.when(zt < zq)
            def _():
                tile(which, cc, zt, False)

            if s in (1, 3):

                @pl.when(zt == zq)
                def _():
                    tile(which, cc, zt, True)

            return carry

        lax.fori_loop(first, last, step, 0)

    def attend_first(cc):
        @pl.when(early)
        def _():
            tile(1, cc, z, False)

        @pl.when(jnp.logical_not(early))
        def _():
            tile(0, cc, z, True)

    def attend_last():
        def step(cc, carry):
            @pl.when(early)
            def _():
                tile(0, cc, z, True)

            return carry

        lax.fori_loop(0, 2, step, 0)

    def events_a(t):
        if t + 1 <= 4:
            for i in range(2):
                b_z(i, t + 1)
        a_z(0, t)

    def events_b(t):
        a_z(1, t)
        dd_send(0, t)
        if t + 1 <= 4:
            for i in range(2):
                b_x1(i, t + 1)
        for i in range(2):
            b_x2(i, t)
        dd_send(1, t)

    pairs = ((wk_h, wk), (wv_h, wv), (wq_h, wq), (wa_h, wa), (wb_h, wb), (wc_h, wc), (wo_h, wo))
    loads = [pltpu.make_async_copy(src, dst, w_sem.at[i]) for i, (src, dst) in enumerate(pairs)]
    own_rows = pltpu.make_async_copy(tok, rows.at[y], own_sem)
    own_rows.start()
    for load in loads[:2]:
        load.start()
    meet()

    def piece(slot, half):
        return rows.at[slot, pl.ds(half * 32, 32)]

    ypair = ((up, lax.rem(y + 3, NT)), (down, lax.rem(y + 1, NT)))
    for order in range(2):
        for d in range(2):
            half = order if d == 0 else 1 - order
            go(remote(tok.at[pl.ds(half * 32, 32)], piece(y, half), y1s.at[d, half], y1r.at[d, half], ypair[d][0]))
    for load in loads[2:]:
        load.start()
    own_rows.wait()

    def norm_slot(slot):
        value = rows[slot].astype(F32)
        scale = lax.rsqrt(jnp.mean(value * value, axis=1, keepdims=True) + 1e-6)
        normed[pl.ds(pl.multiple_of(slot * 64, 64), 64), :] = (value * scale * gain[...]).astype(BF)

    def dot(weight):
        return jnp.dot(normed[...], weight, preferred_element_type=F32)

    def key_slot(j, slot):
        at_rows = pl.ds(pl.multiple_of(slot * 64, 64), 64)
        norm_slot(slot)
        value = normed[at_rows, :]
        keys = jnp.dot(value, wk[...], preferred_element_type=F32)
        kv[c, j, x, z, :, 128:256] = jnp.dot(value, wv[...], preferred_element_type=F32).astype(BF)
        kv[c, j, x, z, :, 0:128] = half_norm(keys, kg[...])

    for load in loads[:2]:
        load.wait()
    key_slot(0, y)
    m_ref[...] = jnp.full(m_ref.shape, -1e30, F32)
    a_begin(0)
    l_ref[...] = jnp.zeros(l_ref.shape, F32)
    acc[...] = jnp.zeros(acc.shape, F32)
    for d in range(2):
        target, source = ypair[d]
        ref = piece(source, d)
        remote(ref, ref, y1s.at[d, d], y1r.at[d, d], target).wait_recv()
        go(remote(ref, ref, y2s.at[d], y2r.at[d], target))
    for d in range(2):
        target, source = ypair[d]
        ref = piece(source, 1 - d)
        remote(ref, ref, y1s.at[d, 1 - d], y1r.at[d, 1 - d], target).wait_recv()
        key_slot(1 + d, source)
        if d == 0:
            a_begin(1)
            a_x1(0)
        else:
            b_begin(0)
    opposite = lax.rem(y + 2, NT)
    for d in range(2):
        ref = piece(opposite, d)
        remote(ref, ref, y2s.at[d], y2r.at[d], ypair[d][0]).wait_recv()
    key_slot(3, opposite)
    b_begin(1)

    def project_q(n, target):
        queries = dot(wq[:, n * 256 : (n + 1) * 256])
        for k in range(2):
            one = half_norm(queries[:, k * 128 : (k + 1) * 128], qg[2 * n + k : 2 * n + k + 1, :])
            target[:, k * 128 : (k + 1) * 128] = one * jnp.asarray(0.125, BF)

    for load in loads[2:5]:
        load.wait()
    project_q(1, q_far)
    q_copy = remote(q_far, q_in, ex_s.at[0], ex_r.at[0], pdev)
    a_x1(1)
    a_x2(0)

    def gate(n):
        span = slice(n * 256, (n + 1) * 256)
        gated[:, span] = (dot(wa[:, span]) * jax.nn.sigmoid(dot(wb[:, span]))).astype(BF)

    gate(0)
    go(q_copy)
    b_z(0, 1)
    b_x1(0, 0)
    gate(1)
    a_x2(1)
    dd_send(0, 0)
    project_q(0, q_own)
    halo_copy = remote(gated.at[pl.ds(224, 32)], halo, ex_s.at[1], ex_r.at[1], nxt)
    go(halo_copy)
    b_z(1, 1)
    b_x1(1, 0)
    b_x2(0, 0)
    b_x1(0, 1)
    low = lax.broadcasted_iota(jnp.int32, (256, 128), 1) < 64

    def pad(which, source):
        for k in range(2):
            head = source[:, k * 128 : (k + 1) * 128].astype(F32)
            qpad[which, 2 * k] = jnp.where(low, head, 0.0).astype(BF)
            qpad[which, 2 * k + 1] = jnp.where(low, 0.0, head).astype(BF)

    pad(0, q_own)
    b_x2(1, 0)
    dd_send(1, 0)
    q_copy.wait_recv()
    pad(1, q_in)
    attend_first(c)
    b_x1(1, 1)
    events_a(1)
    dd_recv(0)
    attend_first(sib)
    for k in range(4):
        gpad[k, 32:288, :] = gated[:, k * 128 : (k + 1) * 128].astype(F32)
    halo_copy.wait_recv()
    for k in range(4):
        gpad[k, 0:32, :] = jnp.where(sp > 0, halo[:, k * 128 : (k + 1) * 128].astype(F32), 0.0)

    def conv_step(k, carry):
        one, two = carry
        total = jnp.zeros((256, 128), F32)
        lanes = pl.ds(pl.multiple_of(k * 128, 128), 128)
        for j in range(KW):
            total = total + taps[j : j + 1, lanes] * gpad[k, j + 2 : j + 258, :]
        csum[k] = total
        return one + total, two + total * total

    nothing = jnp.zeros((256, 128), F32)
    one, two = lax.fori_loop(0, 4, conv_step, (nothing, nothing))
    lane = lax.broadcasted_iota(jnp.int32, (256, 128), 1)
    stat_out[...] = jnp.where(
        lane == 0, jnp.sum(one, axis=1, keepdims=True), jnp.sum(two, axis=1, keepdims=True)
    )
    for k in range(3):
        go(remote(stat_out, stat_in.at[k], st_s.at[k], st_r.at[k], ydev[k]))
    events_b(1)

    def finish(which, out_ref, log_ref):
        table = jnp.zeros((256, 128), F32)
        for k in range(2):
            outs = []
            for m in range(2):
                total = jnp.sum(l_ref[which, 2 * k + m], axis=1, keepdims=True)
                outs.append(acc[which, 2 * k + m] / total)
                table = jnp.where(lane == 2 * k + m, m_ref[which, 2 * k + m] + jnp.log(total), table)
            row = 2 * which + k
            diff = outs[0] - lam[row] * outs[1]
            scale = lax.rsqrt(jnp.mean(diff * diff, axis=1, keepdims=True) + 1e-6)
            out_ref[:, k * 128 : (k + 1) * 128] = (diff * scale * sub_gain[...]).astype(BF)
        log_ref[...] = table.T[0:8, :]

    back = [
        remote(ret_out, ret_in, ex_s.at[2], ex_r.at[2], pdev),
        remote(log_out, log_in, ex_s.at[3], ex_r.at[3], pdev),
    ]

    def send_back(now):
        @pl.when(now)
        def _():
            finish(1, ret_out, log_out)
            for copy in back:
                copy.start()

    done_by_three = lax.rem(z, 4) >= 2
    def close_conv():
        for k in range(3):
            remote(stat_out, stat_in.at[k], st_s.at[k], st_r.at[k], ydev[k]).wait_recv()
        total = (stat_out[...] + stat_in[0]) + (stat_in[1] + stat_in[2])
        mean = total[:, 0:1] / (NT * 512)
        mean_sq = total[:, 1:2] / (NT * 512)
        scale = lax.rsqrt(mean_sq - mean * mean + 1e-5)
        for k in range(4):
            span = slice(k * 128, (k + 1) * 128)
            conv_out[:, span] = jax.nn.silu((csum[k] - mean) * scale * ln_gain[:, span]).astype(BF)
        for load in loads[5:]:
            load.wait()
        for n in range(4):
            span = pl.ds(n * 512, 512)
            part[:, span] = jnp.dot(conv_out[...], wc[:, span], preferred_element_type=F32)

    for t in range(1, 4):
        events_a(t + 1)
        dd_recv(t)
        attend(t, 0)
        events_b(t + 1)
        attend(t, 1)
        if t == 1:
            close_conv()
    send_back(done_by_three)
    dd_recv(4)
    attend(4, 0, 0, 2)
    send_back(jnp.logical_not(done_by_three))
    attend(4, 0, 2, 4)
    attend_last()
    finish(0, attn, log_self)
    for n in range(4):
        span = pl.ds(n * 512, 512)
        part[:, span] += jnp.dot(attn[...], wo[0:256, span], preferred_element_type=F32)
    for copy in back:
        copy.wait_recv()
    for which, table in ((0, log_self), (1, log_in)):
        for k in range(2):
            for m in range(2):
                logs[m, 2 * which + k : 2 * which + k + 1, :] = table[2 * k + m : 2 * k + m + 1, :]

    targets = (up, down)
    blocks = (lax.rem(y + 1, NT), lax.rem(y + 3, NT))

    def block_rows(block):
        return pl.ds(pl.multiple_of(block * 64, 64), 64)

    for n in range(4):
        span = pl.ds(n * 512, 512)
        part[:, span] += jnp.dot(ret_in[...], wo[256:512, span], preferred_element_type=F32)
        if n % 2 == 1:
            d = n // 2
            wide = pl.ds(d * 1024, 1024)
            far[d] = part[block_rows(opposite), wide].astype(BF)
            near[d] = part[block_rows(blocks[1 - d]), wide].astype(BF)
            go(remote(far.at[d], r1.at[d], o1s.at[d], o1r.at[d], targets[d]))
            go(remote(near.at[d], r2.at[1 - d, d], o2s.at[1 - d, d], o2r.at[1 - d, d], targets[1 - d]))
    for d in range(2):
        remote(far.at[d], r1.at[d], o1s.at[d], o1r.at[d], targets[d]).wait_recv()
        wide = pl.ds(d * 1024, 1024)
        total_out[d] = (part[block_rows(blocks[d]), wide] + r1[d].astype(F32)).astype(BF)
        go(remote(total_out.at[d], r2.at[d, d], o2s.at[d, d], o2r.at[d, d], targets[d]))
    for d in (1, 0):
        for k in (1 - d, d):
            remote(total_out.at[d], r2.at[k, d], o2s.at[k, d], o2r.at[k, d], targets[k]).wait_recv()
        wide = pl.ds(d * 1024, 1024)
        mixed[:, wide] = (part[block_rows(y), wide] + (r2[0, d].astype(F32) + r2[1, d].astype(F32))).astype(BF)
    for copy in [*sends, *back]:
        copy.wait_send()
    all_sent()


def on_device(
    tokens, norm_gain, w_glu_a, w_glu_b, conv_taps, ln_gain, w_query, w_key, w_value,
    query_gain, key_gain, lam_head, sub_gain, w_out_conv, w_out_attn,
):
    dma = pltpu.SemaphoreType.DMA

    def vm(*shape, dtype=BF):
        return pltpu.VMEM(shape, dtype)

    return pl.pallas_call(
        layer_kernel,
        out_shape=(jax.ShapeDtypeStruct((64, 2048), BF), jax.ShapeDtypeStruct((2, 4, 256), F32)),
        in_specs=[VM, VM, HBM, HBM, HBM, HBM, HBM, VM, VM, VM, VM, SM, VM, HBM, HBM],
        out_specs=(VM, VM),
        scratch_shapes=[
            vm(4, 64, 2048), vm(256, 2048),
            vm(2048, 512), vm(2048, 512), vm(2048, 512), vm(2048, 128), vm(2048, 128),
            vm(512, 2048), vm(512, 2048),
            vm(256, 512), vm(256, 256), vm(256, 256),
            vm(2, 4, NX, NZ, 64, 256), vm(256, 256), vm(2, 4, 256, 128),
            vm(2, 4, 256, 128, dtype=F32), vm(2, 4, 256, 128, dtype=F32), vm(2, 4, 256, 128, dtype=F32),
            vm(32, 512), vm(4, 288, 128, dtype=F32), vm(4, 256, 128, dtype=F32),
            vm(256, 128, dtype=F32), vm(3, 256, 128, dtype=F32),
            vm(256, 256), vm(256, 512), vm(256, 256), vm(256, 256),
            vm(8, 256, dtype=F32), vm(8, 256, dtype=F32), vm(8, 256, dtype=F32),
            vm(256, 2048, dtype=F32), vm(2, 64, 1024), vm(2, 64, 1024), vm(2, 64, 1024), vm(2, 64, 1024),
            vm(2, 2, 64, 1024),
            dma((7,)), dma, dma((2, 2)), dma((2, 2)), dma((2,)), dma((2,)),
            dma, dma((2, 2)),
            dma, dma((2, 4, 2)),
            dma, dma((2, 4, 2)),
            dma, dma((2, 5, 2, 2)),
            dma, dma((5, 2)),
            dma((4,)), dma((4,)),
            dma((3,)), dma((3,)),
            dma((2,)), dma((2,)), dma((2, 2)), dma((2, 2)),
        ],
        compiler_params=pltpu.CompilerParams(
            collective_id=0, has_side_effects=True, vmem_limit_bytes=53 * 1024 * 1024
        ),
        name="layer",
    )(
        tokens, norm_gain.reshape(1, -1), w_glu_a, w_glu_b, w_query, w_key, w_value, query_gain, key_gain,
        conv_taps, ln_gain.reshape(1, -1), lam_head, sub_gain.reshape(1, -1), w_out_conv, w_out_attn,
    )


def solution(mesh):
    return jax.shard_map(
        on_device,
        mesh=mesh,
        in_specs=(
            P(("sp", "tp"), None), P(), P(None, "tp"), P(None, "tp"), P(None, "tp"), P("tp"),
            P(None, "tp"), P(None, "tp"), P(None, "tp"), P("tp", None), P("tp", None), P("tp"),
            P(), P("tp", None), P("tp", None),
        ),
        out_specs=(P(("sp", "tp"), None), P(None, "tp", "sp")),
        check_vma=False,
    )
```
